512 devices in a mesh: sp: 32 (over z, core), tp: 16 (over y, x).
Axes of the slice: x: 4, y: 4, z: 16, core: 2. Of those that a mesh axis runs over, the one named last changes fastest.
Arguments:
- layer_input: bfloat16 [8192, 2048], P('sp', 'tp'), may hold values from -6 to 6
- doc_ids: int32 [8192], P('sp'), may hold values from 0 to 7, never falling along the last dimension, each value on 1 to 1536 neighbouring positions
- routes: int32 [8192, 2], P('sp'), may hold values from 0 to 31, all different within a row; in each aligned block of 256 rows (0 to 255, 256 to 511, ...) at most 22 rows name the same one
- route_weight: float32 [8192, 2], P('sp'), may hold values from 0.2 to 2
- pool_weight: bfloat16 [4, 512, 512], replicated, may hold values from -0.25 to 0.25
- pool_scale: float32 [2048], replicated, may hold values from 0.1 to 1.9
- norm1_gain: float32 [2048], replicated, may hold values from 0.3 to 3
- norm1_bias: float32 [2048], replicated, may hold values from -3 to 3
- expert_gate: bfloat16 [32, 2048, 2048], P('sp', None, 'tp'), may hold values from -0.125 to 0.125
- expert_up: bfloat16 [32, 2048, 2048], P('sp', None, 'tp'), may hold values from -0.125 to 0.125
- expert_down: bfloat16 [32, 2048, 2048], P('sp', 'tp'), may hold values from -0.125 to 0.125
- shared_gate: bfloat16 [2048, 1024], P(None, 'tp'), may hold values from -0.125 to 0.125
- shared_up: bfloat16 [2048, 1024], P(None, 'tp'), may hold values from -0.125 to 0.125
- shared_down: bfloat16 [1024, 2048], P('tp'), may hold values from -0.1875 to 0.1875
- norm2_gain: float32 [2048], P('tp'), may hold values from 0.1 to 1.9
- norm2_bias: float32 [2048], P('tp'), may hold values from -3 to 3
Outputs:
- settled: bfloat16 [8192, 2048], P('sp', 'tp')
The draws below stay inside these ranges and needn't reach their ends.
Inputs may be any that keep to these rules, and one draw needn't show every extreme that they name: `routes`: in each aligned block of 256 rows no expert is named by more than 22 picks, a bound that some block reaches. `doc_ids`: never falling along the positions; each document spans 1 to 1536 positions.
All inputs are finite; a program needn't handle non-finite values.
Results may differ from the reference program's by a relative error of at most 0.013.
Values may be sent and summed in bfloat16 or wider, within the bound.
A program may use at most 64 MiB of HBM per device.

```python
import math
import jax
import jax.numpy as jnp
import numpy as np
from jax import lax

D = 2048
GROUPS = 4
GROUP_WIDTH = 512
EXPERT_WIDTH = 2048
SHARED_WIDTH = 1024
TOP_K = 2
TOK_DEV = 256
TOKENS = 8192
EXPERTS = 32
CAPACITY = 22
N_SP = 32
N_TP = 16


def levels(stream_key, dims, cuts, low, top_value):
    level = 1.0
    for axis_at, shards_of in cuts:
        steps = jax.random.uniform(jax.random.fold_in(jax.random.fold_in(stream_key, 6), axis_at), (shards_of,), jnp.float32, low / len(cuts), top_value / len(cuts))
        level = level * jnp.repeat(jnp.exp(steps), dims[axis_at] // shards_of).reshape((-1,) + (1,) * (len(dims) - 1 - axis_at))
    return level


def profile(amount, total, reach, slope):
    weights = [(1 << 20) // math.isqrt(standing ** slope) + 1 for standing in range(2, amount + 1)]
    rest, holding = total - reach - (amount - 1), [1] * (amount - 1)
    while rest > 0:
        movable = [i for i in range(amount - 1) if holding[i] < reach]
        mass, budget = sum([weights[i] for i in movable]), rest
        for i in movable:
            extra = min(reach - holding[i], max(1, budget * weights[i] // mass), rest)
            holding[i] = holding[i] + extra
            rest = rest - extra
    return np.array([reach] + holding)


def uneven_parts(own_key, number_of, total, most, slope):
    if number_of == 2:
        one = jax.random.randint(own_key, (), max(1, total - most), min(most, total - 1) + 1)
        return jnp.stack([one, total - one])
    sizes = jnp.asarray(profile(number_of, total, most, slope), jnp.int32)
    couples = (number_of - 1) // 2
    donor, sink = sizes[1:1 + 2 * couples:2], sizes[2:2 + 2 * couples:2]
    slack = jnp.minimum(donor - 1, most - sink)
    moved = jax.random.randint(jax.random.fold_in(own_key, 1), (couples,), 0, 1 << 20) % (slack + 1)
    sizes = sizes.at[1:1 + 2 * couples:2].set(donor - moved).at[2:2 + 2 * couples:2].set(sink + moved)
    return sizes[jax.random.permutation(jax.random.fold_in(own_key, 2), number_of)]


def routed_block(stream_key, own, number, rows, amount, top, bound, lean):
    sequence = jax.random.permutation(stream_key, amount)
    packed, common = load_shares(amount, rows * top, bound, lean, True), load_shares(amount, rows * top, bound, lean, False)
    places = jnp.arange(amount)

    def named(sizes, rotation):
        used = int((sizes > 0).sum())
        fixed = max(1, used // 4)
        moved = fixed + (places - fixed + rotation * (used - fixed)) % max(1, amount - fixed)
        return jnp.zeros((amount,), jnp.int32).at[sequence[jnp.where(places < fixed, places, moved)]].set(jnp.asarray(sizes, jnp.int32))

    sizes = jnp.where(number % 4 == 0, named(packed, number // 4), named(common, number - number // 4 - 1))
    mixed = jax.random.permutation(jax.random.fold_in(own, 3), amount)
    donor, taker = mixed[0:amount // 2 * 2:2], mixed[1:amount // 2 * 2:2]
    slack = jnp.minimum(sizes[donor] - 1, bound - sizes[taker]) // 2
    slack = jnp.where((donor == sequence[0]) | (taker == sequence[0]) | (sizes[taker] == 0), 0, jnp.maximum(slack, 0))
    moved = jax.random.randint(jax.random.fold_in(own, 4), (amount // 2,), 0, 1 << 20) % (slack + 1)
    sizes = sizes.at[donor].add(-moved).at[taker].add(moved)
    items = jnp.searchsorted(jnp.cumsum(sizes), jnp.arange(rows * top), side="right").astype(jnp.int32)
    listing = items.reshape(top, rows).T
    listing = listing[jax.random.permutation(jax.random.fold_in(own, 1), rows)]
    rotation = jax.random.randint(jax.random.fold_in(own, 2), (rows, 1), 0, top)
    return jnp.take_along_axis(listing, (jnp.arange(top)[None, :] + rotation) % top, axis=1)


def load_shares(number_of, total, reach, slope, full):
    portions = [(1 << 20) // math.isqrt(grade ** slope) + 1 for grade in range(1, number_of + 1)]
    largest = reach if full else min(reach, max(-(-total // number_of), total * portions[0] // sum(portions)))
    least = 1 if total - largest >= number_of - 1 else 0
    holding, spare = [largest] + [least] * (number_of - 1), total - largest - least * (number_of - 1)
    while spare > 0:
        movable = [i for i in range(1, number_of) if holding[i] < largest] or [i for i in range(1, number_of) if holding[i] < reach]
        pool, budget = sum([portions[i] for i in movable]), spare
        for i in movable:
            addition = min(reach - holding[i], max(1, budget * portions[i] // pool), spare)
            holding[i] = holding[i] + addition
            spare = spare - addition
    return np.array(holding)


def noise(rng, extent, deviation, limit, cuts=(), kind=jnp.bfloat16):
    loudness = levels(rng, extent, cuts, -0.22, 0.18) if cuts else 1.0
    array = jax.random.normal(rng, extent, jnp.float32) * deviation * loudness
    return jnp.minimum(jnp.maximum(array, -limit), limit).astype(kind)


def setup_inputs(seed: int = 0) -> dict:
    key_list = jax.random.split(jax.random.key(seed), 17)
    layer_input = noise(key_list[0], (TOKENS, D), 1.0, 6.0, ((0, 32), (1, 16)))
    doc_ids = jnp.searchsorted(jnp.cumsum(uneven_parts(key_list[1], N_SP // 4, TOKENS, 6 * TOK_DEV, 2)), jnp.arange(TOKENS), side="right").astype(jnp.int32)
    routes_keys = jax.random.split(jax.random.fold_in(key_list[2], 1), TOKENS // TOK_DEV)
    routes_turns = jax.random.permutation(jax.random.fold_in(key_list[2], 3), TOKENS // TOK_DEV)
    routes = jax.vmap(lambda own, number: routed_block(jax.random.fold_in(key_list[2], 2), own, number, TOK_DEV, EXPERTS, TOP_K, CAPACITY, 2))(routes_keys, routes_turns).reshape((TOKENS, TOP_K))
    route_weight = jnp.clip(jnp.exp(math.log(2.0) - 2.3025851 * jax.random.uniform(key_list[3], (TOKENS, TOP_K), jnp.float32) ** levels(key_list[3], (TOKENS, TOP_K), ((0, 32),), -0.2, 0.2)), 0.2, 2.0)
    pool_weight = noise(key_list[4], (GROUPS, GROUP_WIDTH, GROUP_WIDTH), GROUP_WIDTH ** -0.5, 0.25)
    pool_scale = jnp.clip(1.0 + 0.18 * jax.random.normal(key_list[5], (D,), jnp.float32), 0.1, 1.9)
    norm1_gain = jnp.clip(jnp.exp(jax.random.uniform(key_list[6], (D,), jnp.float32, math.log(0.3), math.log(3.0))), 0.3, 3.0)
    norm1_bias = noise(key_list[7], (D,), 0.5, 3.0, (), jnp.float32)
    expert_gate = noise(key_list[8], (EXPERTS, D, EXPERT_WIDTH), D ** -0.5, 0.125, ((0, 32), (2, 16)))
    expert_up = noise(key_list[9], (EXPERTS, D, EXPERT_WIDTH), D ** -0.5, 0.125, ((0, 32), (2, 16)))
    expert_down = noise(key_list[10], (EXPERTS, EXPERT_WIDTH, D), EXPERT_WIDTH ** -0.5, 0.125, ((0, 32), (1, 16)))
    shared_gate = noise(key_list[11], (D, SHARED_WIDTH), D ** -0.5, 0.125, ((1, 16),))
    shared_up = noise(key_list[12], (D, SHARED_WIDTH), D ** -0.5, 0.125, ((1, 16),))
    shared_down = noise(key_list[13], (SHARED_WIDTH, D), SHARED_WIDTH ** -0.5, 0.1875, ((0, 16),))
    norm2_gain = jnp.clip(1.0 + 0.18 * jax.random.normal(key_list[14], (D,), jnp.float32), 0.1, 1.9)
    norm2_bias = noise(key_list[15], (D,), 0.5, 3.0, ((0, 16),), jnp.float32)
    return dict(layer_input=layer_input, doc_ids=doc_ids, routes=routes, route_weight=route_weight, pool_weight=pool_weight, pool_scale=pool_scale, norm1_gain=norm1_gain, norm1_bias=norm1_bias, expert_gate=expert_gate, expert_up=expert_up, expert_down=expert_down, shared_gate=shared_gate, shared_up=shared_up, shared_down=shared_down, norm2_gain=norm2_gain, norm2_bias=norm2_bias)


WINDOWS = (2, 4, 8, 16)
HALO_ROWS = 15
RESIDUAL_SCALE = 2.0 ** 0.5
NORM_EPS = 1e-05

def pooled_groups(extended, marks, halo_rows):
    length = extended.shape[0] - halo_rows
    group_width = extended.shape[1] // len(WINDOWS)
    own_mark = marks[halo_rows:]
    values = extended.astype(jnp.float32)
    outputs = []
    for group_index, window in enumerate(WINDOWS):
        section = values[:, group_index * group_width:(group_index + 1) * group_width]
        running = jnp.zeros((length, group_width), jnp.float32)
        members = jnp.zeros((length, 1), jnp.float32)
        for offset in range(window):
            first_row = halo_rows - offset
            inside = (marks[first_row:first_row + length] == own_mark).astype(jnp.float32)[:, None]
            running = running + inside * section[first_row:first_row + length]
            members = members + inside
        outputs.append(running / members - section[halo_rows:])
    return jnp.concatenate(outputs, axis=1).astype(jnp.bfloat16)

def layer_norm_rows(values, gain, bias):
    row_mean = lax.optimization_barrier(jnp.mean(values, axis=1, keepdims=True))
    row_var = lax.optimization_barrier(jnp.mean(values * values, axis=1, keepdims=True)) - row_mean * row_mean
    return (values - row_mean) * lax.rsqrt(row_var + NORM_EPS) * gain + bias

def blockwise_down(hidden, down_weight, pieces):
    piece_width = hidden.shape[1] // pieces

    def add_piece(piece_index, running):
        begin = piece_index.astype(jnp.int32) * piece_width
        part_hidden = lax.dynamic_slice_in_dim(hidden, begin, piece_width, 1)
        part_down = lax.dynamic_slice_in_dim(down_weight, begin, piece_width, 0)
        product = jnp.dot(part_hidden, part_down, preferred_element_type=jnp.float32)
        return running + lax.optimization_barrier(product.astype(jnp.bfloat16)).astype(jnp.float32)
    start_value = jnp.zeros((hidden.shape[0], down_weight.shape[1]), jnp.float32)
    return lax.fori_loop(0, pieces, add_piece, start_value)

def reference(layer_input, doc_ids, routes, route_weight, pool_weight, pool_scale, norm1_gain, norm1_bias, expert_gate, expert_up, expert_down, shared_gate, shared_up, shared_down, norm2_gain, norm2_bias):
    extended = jnp.concatenate([jnp.zeros((HALO_ROWS, D), jnp.bfloat16), layer_input], axis=0)
    marks = jnp.concatenate([jnp.zeros((HALO_ROWS,), jnp.float32), (doc_ids + 1).astype(jnp.float32)])
    mixed = pooled_groups(extended, marks, HALO_ROWS)
    projected = jnp.einsum('tgc,gcd->tgd', mixed.reshape(TOKENS, GROUPS, GROUP_WIDTH).astype(jnp.float32), pool_weight.astype(jnp.float32)).reshape(TOKENS, D)
    first = RESIDUAL_SCALE * layer_input.astype(jnp.float32) + projected * pool_scale
    normed = layer_norm_rows(first, norm1_gain, norm1_bias).astype(jnp.bfloat16)
    picks = routes.reshape(N_SP, TOK_DEV * TOP_K).astype(jnp.int32)
    one_hot = (picks[:, :, None] == jnp.arange(EXPERTS, dtype=jnp.int32)[None, None, :]).astype(jnp.int32)
    ranks = lax.optimization_barrier(jnp.sum((jnp.cumsum(one_hot, axis=1) - one_hot) * one_hot, axis=2)).astype(jnp.int32)
    block_index = jnp.broadcast_to(jnp.arange(N_SP, dtype=jnp.int32)[:, None], picks.shape)
    source_rows = jnp.repeat(normed.reshape(N_SP, TOK_DEV, D), TOP_K, axis=1)
    slots = jnp.zeros((EXPERTS, N_SP, CAPACITY, D), jnp.bfloat16).at[picks, block_index, ranks].set(source_rows)

    def run_expert(operands):
        rows_in, gate_w, up_w, down_w = operands
        slot_rows = rows_in.reshape(N_SP * CAPACITY, D)
        gate_part = jnp.dot(slot_rows, gate_w, preferred_element_type=jnp.float32)
        up_part = jnp.dot(slot_rows, up_w, preferred_element_type=jnp.float32)
        hidden = (jax.nn.silu(gate_part) * up_part).astype(jnp.bfloat16)
        return blockwise_down(hidden, down_w, N_TP).astype(jnp.bfloat16).reshape(N_SP, CAPACITY, D)
    routed = lax.map(run_expert, (slots, expert_gate, expert_up, expert_down))
    returned = routed[picks, block_index, ranks].astype(jnp.float32).reshape(TOKENS, TOP_K, D)
    routed_mix = lax.optimization_barrier(jnp.sum(returned * route_weight[:, :, None], axis=1))
    shared_hidden = (jax.nn.silu(jnp.dot(normed, shared_gate, preferred_element_type=jnp.float32)) * jnp.dot(normed, shared_up, preferred_element_type=jnp.float32)).astype(jnp.bfloat16)
    shared = blockwise_down(shared_hidden, shared_down, N_TP)
    second = RESIDUAL_SCALE * normed.astype(jnp.float32) + routed_mix + shared
    return layer_norm_rows(second, norm2_gain, norm2_bias).astype(jnp.bfloat16)
```

```python
import functools

import jax
import jax.numpy as jnp
from jax import lax
from jax.experimental import pallas as pl
from jax.experimental.pallas import tpu as pltpu
from jax.sharding import PartitionSpec as P

MESH = pl.DeviceIdType.MESH
WINDOWS = (2, 4, 8, 16)
RESIDUAL_SCALE = 2.0**0.5
NORM_EPS = 1e-05

SP = 32
TP = 16
TOK = 256
LANES = 128
D = 2048
GROUP = 512
HALO = 16
SHARED = 64
CAP = 22
SLOT = 24
PACKED = SP * SLOT
ROWS = PACKED
PADDED = PACKED + 8

F32 = jnp.float32
BF16 = jnp.bfloat16


def iota(shape, dim):
    return lax.broadcasted_iota(jnp.int32, shape, dim)


def dot(a, b):
    return jnp.dot(a, b, preferred_element_type=F32)


def dot_nt(a, b):
    return lax.dot_general(a, b, (((1,), (1,)), ((), ())), preferred_element_type=F32)


class Gather:
    def __init__(self, buf, cuts, tp, send_sem, recv_sem):
        self.buf, self.cuts, self.tp = buf, cuts, tp
        self.send_sem, self.recv_sem = send_sem, recv_sem
        self.copies = {}

    def at(self, colour, a, b):
        y, x = self.tp // 4, lax.rem(self.tp, 4)
        dx, dy = (a, b) if colour == 0 else (b, a)
        return lax.rem(y + dy + 4, 4) * 4 + lax.rem(x + dx + 4, 4)

    def rows(self, colour, part):
        r0, r1, r2 = self.cuts[2 * colour : 2 * colour + 3]
        lo, hi = {"all": (r0, r2), "lo": (r0, r1), "hi": (r1, r2)}[part]
        return pl.ds(lo, hi - lo)

    def send(self, key, colour, block, part, to):
        number = len(self.copies)
        ref = self.buf.at[block, self.rows(colour, part)]
        copy = pltpu.make_async_remote_copy(
            src_ref=ref,
            dst_ref=ref,
            send_sem=self.send_sem.at[number],
            recv_sem=self.recv_sem.at[number],
            device_id={"tp": to},
            device_id_type=MESH,
        )
        copy.start()
        self.copies[key] = copy

    def arrived(self, *key):
        self.copies[key].wait_recv()

    def first_hop(self, c, a):
        for way in (1, -1):
            self.send(("b1", c, a, way), c, self.at(c, a, 0), "all", self.at(c, 0, way))

    def second_hop(self, c, a):
        for way, part in ((1, "lo"), (-1, "hi")):
            self.arrived("b1", c, a, way)
            block = self.at(c, a, -way)
            self.send(("b2", c, a, way), c, block, part, self.at(c, 0, way))

    def start(self):
        for c in (0, 1):
            for way in (1, -1):
                self.send(("a1", c, way), c, self.tp, "all", self.at(c, way, 0))
        for c in (0, 1):
            self.first_hop(c, 0)

    def finish(self):
        for c in (0, 1):
            for way, part in ((1, "lo"), (-1, "hi")):
                self.arrived("a1", c, way)
                self.send(("a2", c, way), c, self.at(c, -way, 0), part, self.at(c, way, 0))
        for c in (0, 1):
            self.first_hop(c, -1)
            self.first_hop(c, 1)
        for c in (0, 1):
            self.second_hop(c, 0)
        for c in (0, 1):
            self.arrived("a2", c, 1)
            self.arrived("a2", c, -1)
            self.first_hop(c, 2)
        for c in (0, 1):
            self.second_hop(c, -1)
            self.second_hop(c, 1)
        for c in (0, 1):
            self.second_hop(c, 2)
        for c in (0, 1):
            for a in (0, -1, 1, 2):
                self.arrived("b2", c, a, 1)
                self.arrived("b2", c, a, -1)

    def drain(self):
        for copy in self.copies.values():
            copy.wait_send()


def layer(
    docs, routes, weights, scale, gain1, bias1, gain2, bias2,
    x_hbm, pool_hbm, gate_hbm, up_hbm, down_hbm, sgate_hbm, sup_hbm, sdown_hbm,
    out,
    x_buf, halo, halo_docs, first, normed, slots, arrived, arrivals, hidden, shared,
    back, returned, stats, pool_w, expert_w, shared_w, down_w, sdown_w,
    load_sem, barrier_sems, g1s, g1r, g2s, g2r, g3s, g3r, g4s, g4r,
    zs, zr, rs, rr, hs, hr, ws, wr, vs, vr, ts, tr, ks, kr,
):
    sp, tp = lax.axis_index("sp"), lax.axis_index("tp")

    def sp_at(d):
        return lax.rem(sp + d, SP)

    def tp_at(d):
        return lax.rem(tp + d, TP)

    loads = [
        (x_hbm, x_buf.at[tp]),
        (pool_hbm, pool_w),
        (gate_hbm.at[0], expert_w.at[:, pl.ds(0, LANES)]),
        (up_hbm.at[0], expert_w.at[:, pl.ds(LANES, LANES)]),
        (sgate_hbm, shared_w.at[pl.ds(0, SHARED)]),
        (sup_hbm, shared_w.at[pl.ds(SHARED, SHARED)]),
        (down_hbm.at[0, :, pl.ds(pl.multiple_of(tp * LANES, LANES), LANES)], down_w.at[tp]),
        (sdown_hbm.at[:, pl.ds(pl.multiple_of(tp * LANES, LANES), LANES)], sdown_w.at[tp]),
    ]
    loads = [pltpu.make_async_copy(s, d, load_sem.at[i]) for i, (s, d) in enumerate(loads)]
    for load in loads:
        load.start()

    barrier = pltpu.get_barrier_semaphore()

    @pl.loop(1, SP)
    def _(d):
        pl.semaphore_signal(barrier, 1, device_id={"sp": sp_at(d)}, device_id_type=MESH)

    @pl.loop(1, TP)
    def _(d):
        pl.semaphore_signal(barrier, 1, device_id={"tp": tp_at(d)}, device_id_type=MESH)

    loads[0].wait()
    pl.semaphore_wait(barrier, SP - 1 + TP - 1)

    def remote(src, dst, send_sem, recv_sem, **to):
        return pltpu.make_async_remote_copy(
            src_ref=src, dst_ref=dst, send_sem=send_sem, recv_sem=recv_sem,
            device_id=to, device_id_type=MESH,
        )

    tail = remote(x_buf.at[tp, pl.ds(TOK - HALO, HALO)], halo.at[tp], ks.at[0], kr.at[0], sp=sp_at(1))
    tail_docs = remote(docs.at[:, pl.ds(LANES, LANES)], halo_docs, ks.at[1], kr.at[1], sp=sp_at(1))
    tail.start()
    tail_docs.start()
    quarter = TOK // 4
    g1 = Gather(x_buf, [quarter * i for i in range(5)], tp, g1s, g1r)
    g1.start()
    tail.wait_recv()

    def halo_copy(d):
        return remote(halo.at[tp], halo.at[tp], hs.at[d], hr.at[d], tp=tp_at(d))

    @pl.loop(1, TP)
    def _(d):
        halo_copy(d).start()

    g1.finish()

    def columns(d):
        return pl.ds(pl.multiple_of(tp_at(d) * LANES, LANES), LANES)

    def down_copy(d):
        return remote(down_hbm.at[0, :, columns(d)], down_w.at[tp], ws.at[d], wr.at[d], tp=tp_at(d))

    def sdown_copy(d):
        return remote(sdown_hbm.at[:, columns(d)], sdown_w.at[tp], vs.at[d], vr.at[d], tp=tp_at(d))

    @pl.loop(1, TP)
    def _(d):
        sdown_copy(d).start()
        down_copy(d).start()

    route_rows = routes[...]
    expert = iota((SP, TOK), 0)
    names = [(route_rows[k : k + 1] == expert).astype(F32) for k in (0, 1)]
    before = (iota((TOK, TOK), 0) < iota((TOK, TOK), 1)).astype(F32).astype(BF16)
    rank = dot((names[0] + names[1]).astype(BF16), before)
    place = expert.astype(F32) * SLOT + rank
    places = [jnp.sum(n * place, axis=0, keepdims=True) for n in names]
    row = iota((PACKED, TOK), 0).astype(F32)
    spread = ((row == places[0]) | (row == places[1])).astype(F32).astype(BF16)

    marks_row = docs[...].astype(F32)
    p, q = iota((TOK, TOK), 0), iota((TOK, TOK), 1)
    marks_col = jnp.sum(jnp.where(p == q, marks_row, 0.0), axis=1, keepdims=True)
    same = (marks_row == marks_col) & (q <= p)
    tail_docs.wait_recv()
    halo_marks = halo_docs[...][:, LANES - HALO :].astype(F32)
    hp, hq = iota((HALO, HALO), 0), iota((HALO, HALO), 1) - HALO
    halo_same = (halo_marks == marks_col[:HALO]) & (sp > 0)
    for load in loads[1:]:
        load.wait()

    @pl.loop(1, TP)
    def _(d):
        halo_copy(d).wait_recv()

    total = jnp.zeros((TOK, 1), F32)
    squares = jnp.zeros((TOK, 1), F32)
    for g, window in enumerate(WINDOWS):
        band = (same & (q > p - window)).astype(F32)
        halo_band = (halo_same & (hq > hp - window)).astype(F32)
        members = jnp.sum(band, axis=1, keepdims=True)
        halo_members = members[:HALO] + jnp.sum(halo_band, axis=1, keepdims=True)
        members = jnp.concatenate([halo_members, members[HALO:]], axis=0)
        values = jnp.concatenate([x_buf[4 * g + i] for i in range(4)], axis=1)
        halo_values = jnp.concatenate([halo[4 * g + i] for i in range(4)], axis=1)
        running = dot(band.astype(BF16), values)
        halo_running = running[:HALO] + dot(halo_band.astype(BF16), halo_values)
        running = jnp.concatenate([halo_running, running[HALO:]], axis=0)
        mixed = (running / members - values.astype(F32)).astype(BF16)
        here = pl.ds(g * GROUP, GROUP)
        projected = dot(mixed, pool_w[g]) * scale[:, here]
        value = RESIDUAL_SCALE * values.astype(F32) + projected
        first[g] = value
        total += jnp.sum(value, axis=1, keepdims=True)
        squares += jnp.sum(value * value, axis=1, keepdims=True)
    mean = total / D
    spreadness = lax.rsqrt(squares / D - mean * mean + NORM_EPS)
    for g in range(4):
        here = pl.ds(g * GROUP, GROUP)
        value = ((first[g] - mean) * spreadness * gain1[:, here] + bias1[:, here]).astype(BF16)
        for i in range(4):
            normed[4 * g + i] = value[:, i * LANES : (i + 1) * LANES]

    own_slots = dot(spread, normed[tp]).astype(BF16)
    slots[pl.ds(0, PACKED)] = own_slots

    def slot_rows(s):
        return pl.ds(pl.multiple_of(s * SLOT, 8), SLOT)

    def slot_copy(d):
        return remote(slots.at[slot_rows(sp_at(d))], arrived.at[slot_rows(sp)], zs.at[d], zr.at[d], sp=sp_at(d))

    @pl.loop(1, SP)
    def _(d):
        slot_copy(d).start()

    tokens = jnp.concatenate([normed[i] for i in range(TP)], axis=1)
    both = dot_nt(tokens, shared_w[...])
    gate_part, up_part = both[:, :SHARED], both[:, SHARED:]
    units = gate_part * jax.nn.sigmoid(gate_part) * up_part
    shared[tp] = jnp.concatenate([units[: TOK // 2], units[TOK // 2 :]], axis=1).astype(BF16)
    g2 = Gather(shared, [32 * i for i in range(5)], tp, g2s, g2r)
    g2.start()
    g2.finish()

    @pl.loop(1, SP)
    def _(d):
        slot_copy(d).wait_recv()

    own = iota((PACKED, 1), 0)
    own = (own >= sp * SLOT) & (own < sp * SLOT + SLOT)
    taken = jnp.where(own, own_slots.astype(F32), arrived[pl.ds(0, PACKED)].astype(F32))
    arrivals[tp] = taken.astype(BF16)
    step = ROWS // 4
    g3 = Gather(arrivals, [step * i for i in range(5)], tp, g3s, g3r)
    g3.start()

    @pl.loop(1, TP)
    def _(d):
        sdown_copy(d).wait_recv()

    shared_units = jnp.concatenate([shared[i] for i in range(TP)], axis=1)
    nothing = jnp.zeros((SHARED, LANES), BF16)
    parts = [sdown_w[i] for i in range(TP)]
    low = jnp.concatenate([r for part in parts for r in (part, nothing)], axis=0)
    high = jnp.concatenate([r for part in parts for r in (nothing, part)], axis=0)
    shared_out = jnp.concatenate([dot(shared_units, low), dot(shared_units, high)], axis=0)
    g3.finish()

    @pl.loop(0, 4)
    def _(i):
        rows = pl.ds(pl.multiple_of(i * step, 16), step)
        u = jnp.concatenate([arrivals[j, rows] for j in range(TP)], axis=1)
        both = dot(u, expert_w[...])
        gate_part = both[:, :LANES]
        hidden[tp, rows] = (gate_part * jax.nn.sigmoid(gate_part) * both[:, LANES:]).astype(BF16)

    g4 = Gather(hidden, [step * i for i in range(5)], tp, g4s, g4r)
    g4.start()
    g4.finish()

    @pl.loop(1, TP)
    def _(d):
        down_copy(d).wait_recv()

    @pl.loop(0, 4)
    def _(i):
        rows = pl.ds(pl.multiple_of(i * step, 16), step)
        units = jnp.concatenate([hidden[j, rows] for j in range(TP)], axis=1)
        back[rows] = dot(units, down_w[...].reshape(D, LANES)).astype(BF16)

    def back_copy(d):
        return remote(back.at[slot_rows(sp_at(d))], returned.at[slot_rows(sp)], rs.at[d], rr.at[d], sp=sp_at(d))

    @pl.loop(1, SP)
    def _(d):
        back_copy(d).start()

    rows8 = jnp.concatenate(places + [weights[...], jnp.zeros((4, TOK), F32)], axis=0)
    cols = jnp.transpose(rows8)
    column = iota((TOK, PACKED), 1).astype(F32)
    picks = jnp.where(column == cols[:, 0:1], cols[:, 2:3], 0.0)
    picks += jnp.where(column == cols[:, 1:2], cols[:, 3:4], 0.0)
    picks_hi = picks.astype(BF16)
    picks_lo = (picks - picks_hi.astype(F32)).astype(BF16)
    base = RESIDUAL_SCALE * normed[tp].astype(F32) + shared_out

    @pl.loop(1, SP)
    def _(d):
        back_copy(d).wait_recv()

    got = jnp.where(own, back[pl.ds(0, PACKED)].astype(F32), returned[pl.ds(0, PACKED)].astype(F32))
    got = got.astype(BF16)
    second = base + (dot(picks_hi, got) + dot(picks_lo, got))

    lane = iota((TOK, LANES), 1)
    total = jnp.sum(second, axis=1, keepdims=True)
    squares = jnp.sum(second * second, axis=1, keepdims=True)
    both = jnp.where(lane == 0, total, jnp.where(lane == 1, squares, 0.0))
    stats[tp] = jnp.transpose(both)[:8]

    def stats_copy(d):
        return remote(stats.at[tp], stats.at[tp], ts.at[d], tr.at[d], tp=tp_at(d))

    @pl.loop(1, TP)
    def _(d):
        stats_copy(d).start()

    @pl.loop(1, TP)
    def _(d):
        stats_copy(d).wait_recv()

    sums = stats[0]
    for i in range(1, TP):
        sums += stats[i]
    sums = jnp.transpose(sums)
    mean = sums[:, 0:1] / D
    var = sums[:, 1:2] / D - mean * mean
    settled = (second - mean) * lax.rsqrt(var + NORM_EPS)
    out[...] = (settled * gain2[...] + bias2[...]).astype(BF16)

    tail.wait_send()
    tail_docs.wait_send()
    for g in (g1, g2, g3, g4):
        g.drain()

    @pl.loop(1, TP)
    def _(d):
        halo_copy(d).wait_send()
        down_copy(d).wait_send()
        sdown_copy(d).wait_send()
        stats_copy(d).wait_send()

    @pl.loop(1, SP)
    def _(d):
        slot_copy(d).wait_send()
        back_copy(d).wait_send()


def shards(
    layer_input, doc_ids, routes, route_weight, pool_weight, pool_scale, norm1_gain, norm1_bias,
    expert_gate, expert_up, expert_down, shared_gate, shared_up, shared_down, norm2_gain, norm2_bias,
):
    vmem = pl.BlockSpec(memory_space=pltpu.VMEM)
    hbm = pl.BlockSpec(memory_space=pl.ANY)
    dma = pltpu.SemaphoreType.DMA
    scratch = [
        pltpu.VMEM((TP, TOK, LANES), BF16),
        pltpu.VMEM((TP, HALO, LANES), BF16),
        pltpu.VMEM((1, LANES), jnp.int32),
        pltpu.VMEM((4, TOK, GROUP), F32),
        pltpu.VMEM((TP, TOK, LANES), BF16),
        pltpu.VMEM((PADDED, LANES), BF16),
        pltpu.VMEM((PADDED, LANES), BF16),
        pltpu.VMEM((TP, ROWS, LANES), BF16),
        pltpu.VMEM((TP, ROWS, LANES), BF16),
        pltpu.VMEM((TP, TOK // 2, LANES), BF16),
        pltpu.VMEM((PADDED, LANES), BF16),
        pltpu.VMEM((PADDED, LANES), BF16),
        pltpu.VMEM((TP, 8, TOK), F32),
        pltpu.VMEM((4, GROUP, GROUP), BF16),
        pltpu.VMEM((D, 2 * LANES), BF16),
        pltpu.VMEM((2 * SHARED, D), BF16),
        pltpu.VMEM((TP, LANES, LANES), BF16),
        pltpu.VMEM((TP, SHARED, LANES), BF16),
        dma((8,)),
        dma((2,)),
    ]
    scratch += [dma((40,))] * 8 + [dma((SP,))] * 4 + [dma((TP,))] * 8 + [dma((2,))] * 2
    return pl.pallas_call(
        layer,
        out_shape=jax.ShapeDtypeStruct((TOK, LANES), BF16),
        in_specs=[vmem] * 8 + [hbm] * 8,
        out_specs=vmem,
        scratch_shapes=scratch,
        compiler_params=pltpu.CompilerParams(
            collective_id=0, has_side_effects=True, vmem_limit_bytes=60 * 1024 * 1024
        ),
    )(
        doc_ids.reshape(1, TOK), routes.T, route_weight.T,
        pool_scale.reshape(1, D), norm1_gain.reshape(1, D), norm1_bias.reshape(1, D),
        norm2_gain.reshape(1, LANES), norm2_bias.reshape(1, LANES),
        layer_input, pool_weight, expert_gate, expert_up, expert_down,
        shared_gate.T, shared_up.T, shared_down,
    )


def solution(mesh):
    placed = (
        P("sp", "tp"), P("sp"), P("sp", None), P("sp", None), P(), P(), P(), P(),
        P("sp", None, "tp"), P("sp", None, "tp"), P("sp", "tp", None),
        P(None, "tp"), P(None, "tp"), P("tp", None), P("tp"), P("tp"),
    )
    return jax.shard_map(
        shards, mesh=mesh, in_specs=placed, out_specs=P("sp", "tp"), check_vma=False
    )
```

```python
import functools

import jax
import jax.numpy as jnp
from jax import lax
from jax.experimental import pallas as pl
from jax.experimental.pallas import tpu as pltpu
from jax.sharding import PartitionSpec as P

MESH = pl.DeviceIdType.MESH
WINDOWS = (2, 4, 8, 16)
RESIDUAL_SCALE = 2.0**0.5
NORM_EPS = 1e-05

SP = 32
TP = 16
TOK = 256
LANES = 128
D = 2048
GROUP = 512
HALO = 16
SHARED = 64
CAP = 22
SLOT = 24
PACKED = SP * SLOT
PADDED = PACKED + 8
NEAR = 8
HALF = SP * CAP // 2
WIDE = PACKED // 2

F32 = jnp.float32
BF16 = jnp.bfloat16


def iota(shape, dim):
    return lax.broadcasted_iota(jnp.int32, shape, dim)


def dot(a, b):
    return jnp.dot(a, b, preferred_element_type=F32)


def dot_nt(a, b):
    return lax.dot_general(a, b, (((1,), (1,)), ((), ())), preferred_element_type=F32)


class Gather:
    def __init__(self, buf, cuts, tp, send_sem, recv_sem):
        self.buf, self.cuts, self.tp = buf, cuts, tp
        self.send_sem, self.recv_sem = send_sem, recv_sem

    def at(self, colour, a, b):
        y, x = self.tp // 4, lax.rem(self.tp, 4)
        dx, dy = (a, b) if colour == 0 else (b, a)
        return lax.rem(y + dy + 4, 4) * 4 + lax.rem(x + dx + 4, 4)

    def rows(self, colour, part):
        r0, r1, r2 = self.cuts[2 * colour : 2 * colour + 3]
        lo, hi = {"all": (r0, r2), "lo": (r0, r1), "hi": (r1, r2)}[part]
        return pl.ds(lo, hi - lo)

    def copy(self, ref, number, to):
        return pltpu.make_async_remote_copy(
            src_ref=ref,
            dst_ref=ref,
            send_sem=self.send_sem.at[0],
            recv_sem=self.recv_sem.at[number],
            device_id={"tp": to},
            device_id_type=MESH,
        )

    def send(self, number, colour, block, part, to):
        self.copy(self.buf.at[block, self.rows(colour, part)], number, to).start()

    def arrived(self, number, blocks):
        self.copy(self.buf.at[pl.ds(0, blocks)], number, self.at(0, 1, 0)).wait_recv()

    def first_hop(self, number, a):
        for c in (0, 1):
            for way in (1, -1):
                self.send(number, c, self.at(c, a, 0), "all", self.at(c, 0, way))

    def second_hop(self, a):
        for c in (0, 1):
            for way, part in ((1, "lo"), (-1, "hi")):
                self.send(5, c, self.at(c, a, -way), part, self.at(c, 0, way))

    def start(self):
        for c in (0, 1):
            for way in (1, -1):
                self.send(0, c, self.tp, "all", self.at(c, way, 0))
        self.first_hop(1, 0)

    def stage(self, number):
        self.arrived(number, (2, 2, 1, 4, 2, 4)[number])
        if number == 0:
            for c in (0, 1):
                for way, part in ((1, "lo"), (-1, "hi")):
                    self.send(2, c, self.at(c, -way, 0), part, self.at(c, way, 0))
            self.first_hop(3, -1)
            self.first_hop(3, 1)
        elif number == 1:
            self.second_hop(0)
        elif number == 2:
            self.first_hop(4, 2)
        elif number == 3:
            self.second_hop(-1)
            self.second_hop(1)
        elif number == 4:
            self.second_hop(2)

    def drain(self):
        self.copy(self.buf.at[pl.ds(0, 15)], 0, self.at(0, 1, 0)).wait_send()


def layer(
    docs, routes, weights, scale, gain1, bias1, gain2, bias2,
    x_hbm, pool_hbm, gate_hbm, up_hbm, down_hbm, sgate_hbm, sup_hbm, sdown_hbm,
    out,
    x_buf, halo, halo_docs, first, normed, slots, arrived,
    near_in, far_in, near_mid, far_mid, shared, back, returned, stats,
    pool_w, expert_w, shared_w, down_w, sdown_w,
    bands, spread, picks_hi, picks_lo, squeeze, widen,
    load_sem, g1s, g1r, g2s, g2r, g3s, g3r, g4s, g4r, g5s, g5r, g6s, g6r,
    z_send, z_recv, t_send, t_recv,
):
    sp, tp = lax.axis_index("sp"), lax.axis_index("tp")

    def sp_at(d):
        return lax.rem(sp + d + SP, SP)

    def tp_at(d):
        return lax.rem(tp + d, TP)

    loads = [
        (x_hbm, x_buf.at[tp]),
        (pool_hbm, pool_w),
        (gate_hbm.at[0], expert_w.at[:, pl.ds(0, LANES)]),
        (up_hbm.at[0], expert_w.at[:, pl.ds(LANES, LANES)]),
        (sgate_hbm, shared_w.at[pl.ds(0, SHARED)]),
        (sup_hbm, shared_w.at[pl.ds(SHARED, SHARED)]),
        (down_hbm.at[0, :, pl.ds(pl.multiple_of(tp * LANES, LANES), LANES)], down_w.at[tp]),
        (sdown_hbm.at[:, pl.ds(pl.multiple_of(tp * LANES, LANES), LANES)], sdown_w.at[tp]),
    ]
    loads = [pltpu.make_async_copy(s, d, load_sem.at[i]) for i, (s, d) in enumerate(loads)]
    for load in loads:
        load.start()

    barrier = pltpu.get_barrier_semaphore()

    @pl.loop(1, SP)
    def _(d):
        pl.semaphore_signal(barrier, 1, device_id={"sp": sp_at(d)}, device_id_type=MESH)

    @pl.loop(1, TP)
    def _(d):
        pl.semaphore_signal(barrier, 1, device_id={"tp": tp_at(d)}, device_id_type=MESH)

    route_rows = routes[...]
    expert = iota((SP, TOK), 0)
    names = [(route_rows[k : k + 1] == expert).astype(F32) for k in (0, 1)]
    before = (iota((TOK, TOK), 0) < iota((TOK, TOK), 1)).astype(F32).astype(BF16)
    rank = dot((names[0] + names[1]).astype(BF16), before)
    order = jnp.bitwise_and(expert - sp + (SP + NEAR), SP - 1)
    place = order.astype(F32) * SLOT + rank
    places = [jnp.sum(n * place, axis=0, keepdims=True) for n in names]
    row = iota((PACKED, TOK), 0).astype(F32)
    spread[...] = ((row == places[0]) | (row == places[1])).astype(F32).astype(BF16)
    rows8 = jnp.concatenate(places + [weights[...], jnp.zeros((4, TOK), F32)], axis=0)
    cols = jnp.transpose(rows8)
    column = iota((TOK, PACKED), 1).astype(F32)
    picks = jnp.where(column == cols[:, 0:1], cols[:, 2:3], 0.0)
    picks += jnp.where(column == cols[:, 1:2], cols[:, 3:4], 0.0)
    high = picks.astype(BF16)
    picks_hi[...] = high
    picks_lo[...] = (picks - high.astype(F32)).astype(BF16)

    tight = iota((HALF, 1), 0).astype(F32)
    tight = tight + 2.0 * jnp.floor((tight + 0.5) * (1.0 / CAP))
    squeeze[...] = (iota((HALF, WIDE), 1).astype(F32) == tight).astype(F32).astype(BF16)
    tight = iota((1, HALF), 1).astype(F32)
    tight = tight + 2.0 * jnp.floor((tight + 0.5) * (1.0 / CAP))
    widen[...] = (iota((WIDE, HALF), 0).astype(F32) == tight).astype(F32).astype(BF16)

    marks_row = docs[...].astype(F32)
    p, q = iota((TOK, TOK), 0), iota((TOK, TOK), 1)
    marks_col = jnp.sum(jnp.where(p == q, marks_row, 0.0), axis=1, keepdims=True)
    same = (marks_row == marks_col) & (q <= p)
    members = []
    for g, window in enumerate(WINDOWS):
        band = (same & (q > p - window)).astype(F32)
        bands[g] = band.astype(BF16)
        members.append(jnp.sum(band, axis=1, keepdims=True))

    loads[0].wait()
    pl.semaphore_wait(barrier, SP - 1 + TP - 1)

    def remote(src, dst, send_sem, recv_sem, **to):
        return pltpu.make_async_remote_copy(
            src_ref=src, dst_ref=dst, send_sem=send_sem, recv_sem=recv_sem,
            device_id=to, device_id_type=MESH,
        )

    def to_all(ref, number):
        def copy(d):
            return remote(ref.at[tp], ref.at[tp], t_send.at[number], t_recv.at[number], tp=tp_at(d))

        return copy

    def all_of(ref, number):
        block = ref.at[pl.ds(0, TP - 1)]
        return remote(block, block, t_send.at[number], t_recv.at[number], tp=tp_at(1))

    tail = remote(
        x_buf.at[tp, pl.ds(TOK - HALO, HALO)], halo.at[tp], t_send.at[4], t_recv.at[4], sp=sp_at(1)
    )
    tail_docs = remote(docs.at[:, pl.ds(LANES, LANES)], halo_docs, t_send.at[5], t_recv.at[5], sp=sp_at(1))
    tail.start()
    tail_docs.start()
    g1 = Gather(x_buf, [64 * i for i in range(5)], tp, g1s, g1r)
    g1.start()
    tail.wait_recv()

    @pl.loop(1, TP)
    def _(d):
        to_all(halo, 0)(d).start()

    tail_docs.wait_recv()
    halo_marks = halo_docs[...][:, LANES - HALO :].astype(F32)
    hp, hq = iota((HALO, HALO), 0), iota((HALO, HALO), 1) - HALO
    halo_same = (halo_marks == marks_col[:HALO]) & (sp > 0)
    for number in range(6):
        g1.stage(number)

    def columns(d):
        return pl.ds(pl.multiple_of(tp_at(d) * LANES, LANES), LANES)

    @pl.loop(1, TP)
    def _(d):
        source = down_hbm.at[0, :, columns(d)]
        remote(source, down_w.at[tp], t_send.at[1], t_recv.at[1], tp=tp_at(d)).start()

    for load in loads[1:]:
        load.wait()
    all_of(halo, 0).wait_recv()

    total = jnp.zeros((TOK, 1), F32)
    squares = jnp.zeros((TOK, 1), F32)
    for g, window in enumerate(WINDOWS):
        halo_band = (halo_same & (hq > hp - window)).astype(F32)
        halo_members = members[g][:HALO] + jnp.sum(halo_band, axis=1, keepdims=True)
        share = 1.0 / jnp.concatenate([halo_members, members[g][HALO:]], axis=0)
        values = jnp.concatenate([x_buf[4 * g + i] for i in range(4)], axis=1)
        halo_values = jnp.concatenate([halo[4 * g + i] for i in range(4)], axis=1)
        running = dot(bands[g], values)
        halo_running = running[:HALO] + dot(halo_band.astype(BF16), halo_values)
        running = jnp.concatenate([halo_running, running[HALO:]], axis=0)
        mixed = (running * share - values.astype(F32)).astype(BF16)
        here = pl.ds(g * GROUP, GROUP)
        projected = dot(mixed, pool_w[g]) * scale[:, here]
        value = RESIDUAL_SCALE * values.astype(F32) + projected
        first[g] = value
        total += jnp.sum(value, axis=1, keepdims=True)
        squares += jnp.sum(value * value, axis=1, keepdims=True)
    mean = total / D
    factor = lax.rsqrt(squares / D - mean * mean + NORM_EPS)
    for g in range(4):
        here = pl.ds(g * GROUP, GROUP)
        value = ((first[g] - mean) * factor * gain1[:, here] + bias1[:, here]).astype(BF16)
        for i in range(4):
            normed[4 * g + i] = value[:, i * LANES : (i + 1) * LANES]

    def block(d):
        return pl.ds(pl.multiple_of(jnp.bitwise_and(d + (SP + NEAR), SP - 1) * SLOT, 8), SLOT)

    def over_sp(source, target, number, first_d, last_d):
        def start(d):
            remote(
                source.at[block(d)], target.at[block(-d)],
                z_send.at[number], z_recv.at[number], sp=sp_at(d),
            ).start()

        pl.loop(max(first_d, 1), last_d)(start)
        if first_d < 0:
            pl.loop(first_d, 0)(start)

    def over_sp_all(ref, number, blocks):
        rows = ref.at[pl.ds(0, blocks * SLOT)]
        return remote(rows, rows, z_send.at[number], z_recv.at[number], sp=sp_at(1))

    own_slots = dot(spread[...], normed[tp]).astype(BF16)
    slots[pl.ds(0, PACKED)] = own_slots
    over_sp(slots, arrived, 0, 1 - NEAR, NEAR + 1)
    over_sp(slots, arrived, 1, NEAR + 1, SP - NEAR + 1)

    tokens = jnp.concatenate([normed[i] for i in range(TP)], axis=1)
    both = dot_nt(tokens, shared_w[...])
    gate_part, up_part = both[:, :SHARED], both[:, SHARED:]
    units = gate_part * jax.nn.sigmoid(gate_part) * up_part
    shared[tp] = jnp.concatenate([units[: TOK // 2], units[TOK // 2 :]], axis=1).astype(BF16)
    g2 = Gather(shared, [32 * i for i in range(5)], tp, g2s, g2r)
    g2.start()

    cuts = [0, 96, 176, 272, HALF]
    mine = NEAR * SLOT
    over_sp_all(arrived, 0, 15).wait_recv()
    taken = jnp.concatenate(
        [arrived[pl.ds(0, mine)], own_slots[mine : mine + SLOT], arrived[pl.ds(mine + SLOT, WIDE - mine - SLOT)]],
        axis=0,
    )
    near_in[tp] = dot(squeeze[...], taken).astype(BF16)
    g3 = Gather(near_in, cuts, tp, g3s, g3r)
    g3.start()
    for number in range(5):
        g3.stage(number)
        g2.stage(number)

    over_sp_all(arrived, 1, 16).wait_recv()
    far_in[tp] = dot(squeeze[...], arrived[pl.ds(WIDE, WIDE)]).astype(BF16)
    g4 = Gather(far_in, cuts, tp, g4s, g4r)
    g4.start()
    g3.stage(5)
    g2.stage(5)

    def run_expert(rows_in, mid):
        @pl.loop(0, 2)
        def _(i):
            rows = pl.ds(pl.multiple_of(i * (HALF // 2), 16), HALF // 2)
            u = jnp.concatenate([rows_in[j, rows] for j in range(TP)], axis=1)
            both = dot(u, expert_w[...])
            gate_part = both[:, :LANES]
            mid[tp, rows] = (gate_part * jax.nn.sigmoid(gate_part) * both[:, LANES:]).astype(BF16)

    run_expert(near_in, near_mid)
    for number in range(5):
        g4.stage(number)

    @pl.loop(1, TP)
    def _(d):
        remote(sdown_hbm.at[:, columns(d)], sdown_w.at[tp], t_send.at[2], t_recv.at[2], tp=tp_at(d)).start()

    g4.stage(5)
    run_expert(far_in, far_mid)

    def run_down(mid, begin):
        units = jnp.concatenate([mid[j] for j in range(TP)], axis=1)
        result = dot(units, down_w[...].reshape(D, LANES)).astype(BF16)
        back[pl.ds(begin, WIDE)] = dot(widen[...], result).astype(BF16)

    g5 = Gather(far_mid, cuts, tp, g5s, g5r)
    g5.start()
    for number in range(5):
        g5.stage(number)
    g6 = Gather(near_mid, cuts, tp, g6s, g6r)
    g6.start()
    g5.stage(5)
    all_of(down_w, 1).wait_recv()
    run_down(far_mid, WIDE)
    over_sp(back, returned, 2, NEAR, SP - NEAR)
    for number in range(6):
        g6.stage(number)
    run_down(near_mid, 0)
    over_sp(back, returned, 3, -NEAR, NEAR)

    all_of(sdown_w, 2).wait_recv()
    shared_units = jnp.concatenate([shared[i] for i in range(TP)], axis=1)
    nothing = jnp.zeros((SHARED, LANES), BF16)
    parts = [sdown_w[i] for i in range(TP)]
    low = jnp.concatenate([r for part in parts for r in (part, nothing)], axis=0)
    high = jnp.concatenate([r for part in parts for r in (nothing, part)], axis=0)
    shared_out = jnp.concatenate([dot(shared_units, low), dot(shared_units, high)], axis=0)
    base = RESIDUAL_SCALE * normed[tp].astype(F32) + shared_out

    over_sp_all(returned, 2, 16).wait_recv()
    over_sp_all(returned, 3, 15).wait_recv()
    got = jnp.concatenate(
        [returned[pl.ds(0, mine)], back[pl.ds(mine, SLOT)], returned[pl.ds(mine + SLOT, PACKED - mine - SLOT)]],
        axis=0,
    )
    second = base + (dot(picks_hi[...], got) + dot(picks_lo[...], got))

    lane = iota((TOK, LANES), 1)
    total = jnp.sum(second, axis=1, keepdims=True)
    squares = jnp.sum(second * second, axis=1, keepdims=True)
    both = jnp.where(lane == 0, total, jnp.where(lane == 1, squares, 0.0))
    stats[tp] = jnp.transpose(both)[:2]

    @pl.loop(1, TP)
    def _(d):
        to_all(stats, 3)(d).start()

    all_of(stats, 3).wait_recv()
    sums = stats[0]
    for i in range(1, TP):
        sums += stats[i]
    sums = jnp.transpose(jnp.concatenate([sums, jnp.zeros((6, TOK), F32)], axis=0))
    mean = sums[:, 0:1] / D
    var = sums[:, 1:2] / D - mean * mean
    settled = (second - mean) * lax.rsqrt(var + NORM_EPS)
    out[...] = (settled * gain2[...] + bias2[...]).astype(BF16)

    tail.wait_send()
    tail_docs.wait_send()
    for g in (g1, g2, g3, g4, g5, g6):
        g.drain()
    for number, ref in enumerate((halo, down_w, sdown_w, stats)):
        all_of(ref, number).wait_send()
    for number, ref, blocks in ((0, slots, 15), (1, slots, 16), (2, back, 16), (3, back, 15)):
        over_sp_all(ref, number, blocks).wait_send()


def shards(
    layer_input, doc_ids, routes, route_weight, pool_weight, pool_scale, norm1_gain, norm1_bias,
    expert_gate, expert_up, expert_down, shared_gate, shared_up, shared_down, norm2_gain, norm2_bias,
):
    vmem = pl.BlockSpec(memory_space=pltpu.VMEM)
    hbm = pl.BlockSpec(memory_space=pl.ANY)
    dma = pltpu.SemaphoreType.DMA
    scratch = [
        pltpu.VMEM((TP, TOK, LANES), BF16),
        pltpu.VMEM((TP, HALO, LANES), BF16),
        pltpu.VMEM((1, LANES), jnp.int32),
        pltpu.VMEM((4, TOK, GROUP), F32),
        pltpu.VMEM((TP, TOK, LANES), BF16),
        pltpu.VMEM((PADDED, LANES), BF16),
        pltpu.VMEM((PADDED, LANES), BF16),
        pltpu.VMEM((TP, HALF, LANES), BF16),
        pltpu.VMEM((TP, HALF, LANES), BF16),
        pltpu.VMEM((TP, HALF, LANES), BF16),
        pltpu.VMEM((TP, HALF, LANES), BF16),
        pltpu.VMEM((TP, TOK // 2, LANES), BF16),
        pltpu.VMEM((PADDED, LANES), BF16),
        pltpu.VMEM((PADDED, LANES), BF16),
        pltpu.VMEM((TP, 2, TOK), F32),
        pltpu.VMEM((4, GROUP, GROUP), BF16),
        pltpu.VMEM((D, 2 * LANES), BF16),
        pltpu.VMEM((2 * SHARED, D), BF16),
        pltpu.VMEM((TP, LANES, LANES), BF16),
        pltpu.VMEM((TP, SHARED, LANES), BF16),
        pltpu.VMEM((4, TOK, TOK), BF16),
        pltpu.VMEM((PACKED, TOK), BF16),
        pltpu.VMEM((TOK, PACKED), BF16),
        pltpu.VMEM((TOK, PACKED), BF16),
        pltpu.VMEM((HALF, WIDE), BF16),
        pltpu.VMEM((WIDE, HALF), BF16),
        dma((8,)),
    ]
    scratch += [dma((1,)), dma((6,))] * 6 + [dma((4,))] * 2 + [dma((6,))] * 2
    return pl.pallas_call(
        layer,
        out_shape=jax.ShapeDtypeStruct((TOK, LANES), BF16),
        in_specs=[vmem] * 8 + [hbm] * 8,
        out_specs=vmem,
        scratch_shapes=scratch,
        compiler_params=pltpu.CompilerParams(
            collective_id=0, has_side_effects=True, vmem_limit_bytes=60 * 1024 * 1024
        ),
    )(
        doc_ids.reshape(1, TOK), routes.T, route_weight.T,
        pool_scale.reshape(1, D), norm1_gain.reshape(1, D), norm1_bias.reshape(1, D),
        norm2_gain.reshape(1, LANES), norm2_bias.reshape(1, LANES),
        layer_input, pool_weight, expert_gate, expert_up, expert_down,
        shared_gate.T, shared_up.T, shared_down,
    )


def solution(mesh):
    placed = (
        P("sp", "tp"), P("sp"), P("sp", None), P("sp", None), P(), P(), P(), P(),
        P("sp", None, "tp"), P("sp", None, "tp"), P("sp", "tp", None),
        P(None, "tp"), P(None, "tp"), P("tp", None), P("tp"), P("tp"),
    )
    return jax.shard_map(
        shards, mesh=mesh, in_specs=placed, out_specs=P("sp", "tp"), check_vma=False
    )
```

```python
import functools

import jax
import jax.numpy as jnp
from jax import lax
from jax.experimental import pallas as pl
from jax.experimental.pallas import tpu as pltpu
from jax.sharding import PartitionSpec as P

MESH = pl.DeviceIdType.MESH
WINDOWS = (2, 4, 8, 16)
RESIDUAL_SCALE = 2.0**0.5
NORM_EPS = 1e-05

SP = 32
TP = 16
TOK = 256
LANES = 128
D = 2048
GROUP = 512
HALO = 16
SHARED = 64
CAP = 22
SLOT = 24
PACKED = SP * SLOT
PADDED = PACKED + 8
BACK = 4
CHUNKS = (
    tuple(range(-4, 4)),
    tuple(range(4, 8)) + tuple(range(-8, -4)),
    tuple(range(8, 12)) + tuple(range(-12, -8)),
    tuple(range(12, 20)),
)
HALF = SP * CAP // 4
WIDE = PACKED // 4
CUTS = ((0, 48, 96, 144, HALF), (0, 48, 80, 128, HALF))
ORDER = (
    "z0 g00 g01 i00",
    "z1 i01 g02 g03",
    "i02 i03 i10 i11",
    "g04 i04 i12 z2",
    "i13 g05 i05 i14",
    "z3 i20 i21 h00",
    "h01 i15 i30 i31",
    "i22 i23 h02 h03",
    "i32 i33 h10 h11",
    "i24 h04 h12 h13",
    "i34 i25 h05 h14",
    "h20 h21 i35 h15",
    "h22 h23 h30 h31",
    "h24 h32 h33 s0",
    "h34 h25 h35",
)

F32 = jnp.float32
BF16 = jnp.bfloat16


def iota(shape, dim):
    return lax.broadcasted_iota(jnp.int32, shape, dim)


def dot(a, b):
    return jnp.dot(a, b, preferred_element_type=F32)


def dot_nt(a, b):
    return lax.dot_general(a, b, (((1,), (1,)), ((), ())), preferred_element_type=F32)


class Gather:
    def __init__(self, buf, cuts, tp, send_sem, recv_sem):
        self.buf, self.cuts, self.tp = buf, cuts, tp
        self.send_sem, self.recv_sem = send_sem, recv_sem

    def at(self, colour, a, b):
        y, x = self.tp // 4, lax.rem(self.tp, 4)
        dx, dy = (a, b) if colour == 0 else (b, a)
        return lax.rem(y + dy + 4, 4) * 4 + lax.rem(x + dx + 4, 4)

    def rows(self, colour, part):
        r0, r1, r2 = self.cuts[2 * colour : 2 * colour + 3]
        lo, hi = {"all": (r0, r2), "lo": (r0, r1), "hi": (r1, r2)}[part]
        return pl.ds(lo, hi - lo)

    def copy(self, ref, number, to):
        return pltpu.make_async_remote_copy(
            src_ref=ref,
            dst_ref=ref,
            send_sem=self.send_sem.at[0],
            recv_sem=self.recv_sem.at[number],
            device_id={"tp": to},
            device_id_type=MESH,
        )

    def send(self, number, colour, block, part, to):
        self.copy(self.buf.at[block, self.rows(colour, part)], number, to).start()

    def arrived(self, number, blocks):
        self.copy(self.buf.at[pl.ds(0, blocks)], number, self.at(0, 1, 0)).wait_recv()

    def first_hop(self, number, a):
        for c in (0, 1):
            for way in (1, -1):
                self.send(number, c, self.at(c, a, 0), "all", self.at(c, 0, way))

    def second_hop(self, a):
        for c in (0, 1):
            for way, part in ((1, "lo"), (-1, "hi")):
                self.send(5, c, self.at(c, a, -way), part, self.at(c, 0, way))

    def start(self):
        for c in (0, 1):
            for way in (1, -1):
                self.send(0, c, self.tp, "all", self.at(c, way, 0))
        self.first_hop(1, 0)

    def stage(self, number):
        self.arrived(number, (2, 2, 1, 4, 2, 4)[number])
        if number == 0:
            for c in (0, 1):
                for way, part in ((1, "lo"), (-1, "hi")):
                    self.send(2, c, self.at(c, -way, 0), part, self.at(c, way, 0))
            self.first_hop(3, -1)
            self.first_hop(3, 1)
        elif number == 1:
            self.second_hop(0)
        elif number == 2:
            self.first_hop(4, 2)
        elif number == 3:
            self.second_hop(-1)
            self.second_hop(1)
        elif number == 4:
            self.second_hop(2)

    def drain(self):
        self.copy(self.buf.at[pl.ds(0, 15)], 0, self.at(0, 1, 0)).wait_send()


def layer(
    docs, routes, weights, scale, gain1, bias1, gain2, bias2,
    x_hbm, pool_hbm, gate_hbm, up_hbm, down_hbm, sgate_hbm, sup_hbm, sdown_hbm,
    out,
    x_buf, halo, halo_docs, first, normed, slots, arrived,
    in0, in1, in2, in3, mid0, mid1, mid2, mid3, shared, back, returned, stats,
    pool_w, expert_w, shared_w, down_w, sdown_w,
    bands, spread, picks_hi, picks_lo, squeeze, widen,
    load_sem, g_send, g_recv, z_send, z_recv, t_send, t_recv,
):
    sp, tp = lax.axis_index("sp"), lax.axis_index("tp")

    def sp_at(d):
        return lax.rem(sp + d + SP, SP)

    def tp_at(d):
        return lax.rem(tp + d, TP)

    loads = [
        (x_hbm, x_buf.at[tp]),
        (pool_hbm, pool_w),
        (gate_hbm.at[0], expert_w.at[:, pl.ds(0, LANES)]),
        (up_hbm.at[0], expert_w.at[:, pl.ds(LANES, LANES)]),
        (sgate_hbm, shared_w.at[pl.ds(0, SHARED)]),
        (sup_hbm, shared_w.at[pl.ds(SHARED, SHARED)]),
        (down_hbm.at[0, :, pl.ds(pl.multiple_of(tp * LANES, LANES), LANES)], down_w.at[tp]),
        (sdown_hbm.at[:, pl.ds(pl.multiple_of(tp * LANES, LANES), LANES)], sdown_w.at[tp]),
    ]
    loads = [pltpu.make_async_copy(s, d, load_sem.at[i]) for i, (s, d) in enumerate(loads)]
    for load in loads:
        load.start()

    barrier = pltpu.get_barrier_semaphore()

    @pl.loop(1, SP)
    def _(d):
        pl.semaphore_signal(barrier, 1, device_id={"sp": sp_at(d)}, device_id_type=MESH)

    @pl.loop(1, TP)
    def _(d):
        pl.semaphore_signal(barrier, 1, device_id={"tp": tp_at(d)}, device_id_type=MESH)

    route_rows = routes[...]
    expert = iota((SP, TOK), 0)
    names = [(route_rows[k : k + 1] == expert).astype(F32) for k in (0, 1)]
    before = (iota((TOK, TOK), 0) < iota((TOK, TOK), 1)).astype(F32).astype(BF16)
    rank = dot((names[0] + names[1]).astype(BF16), before)
    order = jnp.bitwise_and(expert - sp + (SP + BACK), SP - 1)
    place = order.astype(F32) * SLOT + rank
    places = [jnp.sum(n * place, axis=0, keepdims=True) for n in names]
    row = iota((PACKED, TOK), 0).astype(F32)
    spread[...] = ((row == places[0]) | (row == places[1])).astype(F32).astype(BF16)
    rows8 = jnp.concatenate(places + [weights[...], jnp.zeros((4, TOK), F32)], axis=0)
    cols = jnp.transpose(rows8)
    column = iota((TOK, PACKED), 1).astype(F32)
    picks = jnp.where(column == cols[:, 0:1], cols[:, 2:3], 0.0)
    picks += jnp.where(column == cols[:, 1:2], cols[:, 3:4], 0.0)
    high = picks.astype(BF16)
    picks_hi[...] = high
    picks_lo[...] = (picks - high.astype(F32)).astype(BF16)

    tight = iota((HALF, 1), 0).astype(F32)
    tight = tight + 2.0 * jnp.floor((tight + 0.5) * (1.0 / CAP))
    squeeze[...] = (iota((HALF, WIDE), 1).astype(F32) == tight).astype(F32).astype(BF16)
    tight = iota((1, HALF), 1).astype(F32)
    tight = tight + 2.0 * jnp.floor((tight + 0.5) * (1.0 / CAP))
    widen[...] = (iota((WIDE, HALF), 0).astype(F32) == tight).astype(F32).astype(BF16)

    marks_row = docs[...].astype(F32)
    p, q = iota((TOK, TOK), 0), iota((TOK, TOK), 1)
    marks_col = jnp.sum(jnp.where(p == q, marks_row, 0.0), axis=1, keepdims=True)
    same = (marks_row == marks_col) & (q <= p)
    members = []
    for g, window in enumerate(WINDOWS):
        band = (same & (q > p - window)).astype(F32)
        bands[g] = band.astype(BF16)
        members.append(jnp.sum(band, axis=1, keepdims=True))

    loads[0].wait()
    pl.semaphore_wait(barrier, SP - 1 + TP - 1)

    def remote(src, dst, send_sem, recv_sem, **to):
        return pltpu.make_async_remote_copy(
            src_ref=src, dst_ref=dst, send_sem=send_sem, recv_sem=recv_sem,
            device_id=to, device_id_type=MESH,
        )

    def to_all(ref, number):
        def copy(d):
            return remote(ref.at[tp], ref.at[tp], t_send.at[number], t_recv.at[number], tp=tp_at(d))

        return copy

    def all_of(ref, number):
        block = ref.at[pl.ds(0, TP - 1)]
        return remote(block, block, t_send.at[number], t_recv.at[number], tp=tp_at(1))

    tail = remote(
        x_buf.at[tp, pl.ds(TOK - HALO, HALO)], halo.at[tp], t_send.at[4], t_recv.at[4], sp=sp_at(1)
    )
    tail_docs = remote(docs.at[:, pl.ds(LANES, LANES)], halo_docs, t_send.at[5], t_recv.at[5], sp=sp_at(1))
    tail.start()
    tail_docs.start()
    def gather(number, buf, cuts):
        return Gather(buf, cuts, tp, g_send.at[pl.ds(number, 1)], g_recv.at[number])

    g1 = gather(0, x_buf, [64 * i for i in range(5)])
    g1.start()

    def send_down(a, b):
        to = g1.at(0, a, b)
        source = down_hbm.at[0, :, pl.ds(pl.multiple_of(to * LANES, LANES), LANES)]
        remote(source, down_w.at[tp], t_send.at[1], t_recv.at[1], tp=to).start()

    for a, b in ((1, 0), (-1, 0), (0, 1), (0, -1), (1, 1), (-1, -1), (1, -1), (-1, 1)):
        send_down(a, b)
    tail.wait_recv()

    @pl.loop(1, TP)
    def _(d):
        to_all(halo, 0)(d).start()

    tail_docs.wait_recv()
    halo_marks = halo_docs[...][:, LANES - HALO :].astype(F32)
    hp, hq = iota((HALO, HALO), 0), iota((HALO, HALO), 1) - HALO
    halo_same = (halo_marks == marks_col[:HALO]) & (sp > 0)
    for number in range(6):
        g1.stage(number)
        if number == 4:
            for a, b in ((2, 0), (0, 2), (2, 1), (1, 2), (2, -1), (-1, 2), (2, 2)):
                send_down(a, b)

    for load in loads[1:]:
        load.wait()
    all_of(halo, 0).wait_recv()

    total = jnp.zeros((TOK, 1), F32)
    squares = jnp.zeros((TOK, 1), F32)
    for g, window in enumerate(WINDOWS):
        halo_band = (halo_same & (hq > hp - window)).astype(F32)
        halo_members = members[g][:HALO] + jnp.sum(halo_band, axis=1, keepdims=True)
        share = 1.0 / jnp.concatenate([halo_members, members[g][HALO:]], axis=0)
        values = jnp.concatenate([x_buf[4 * g + i] for i in range(4)], axis=1)
        halo_values = jnp.concatenate([halo[4 * g + i] for i in range(4)], axis=1)
        running = dot(bands[g], values)
        halo_running = running[:HALO] + dot(halo_band.astype(BF16), halo_values)
        running = jnp.concatenate([halo_running, running[HALO:]], axis=0)
        mixed = (running * share - values.astype(F32)).astype(BF16)
        here = pl.ds(g * GROUP, GROUP)
        projected = dot(mixed, pool_w[g]) * scale[:, here]
        value = RESIDUAL_SCALE * values.astype(F32) + projected
        first[g] = value
        total += jnp.sum(value, axis=1, keepdims=True)
        squares += jnp.sum(value * value, axis=1, keepdims=True)
    mean = total / D
    factor = lax.rsqrt(squares / D - mean * mean + NORM_EPS)
    for g in range(4):
        here = pl.ds(g * GROUP, GROUP)
        value = ((first[g] - mean) * factor * gain1[:, here] + bias1[:, here]).astype(BF16)
        for i in range(4):
            normed[4 * g + i] = value[:, i * LANES : (i + 1) * LANES]

    def block(d):
        return pl.ds((d + BACK) % SP * SLOT, SLOT)

    def over_sp(source, target, number, ds):
        for d in ds:
            if d != 0:
                remote(
                    source.at[block(d)], target.at[block(-d)],
                    z_send.at[number], z_recv.at[number], sp=sp_at(d),
                ).start()

    def over_sp_all(ref, number):
        rows = ref.at[pl.ds(0, (7 if number % 4 == 0 else 8) * SLOT)]
        return remote(rows, rows, z_send.at[number], z_recv.at[number], sp=sp_at(1))

    def runs(chunk):
        places = [(d + BACK) % SP for d in CHUNKS[chunk]]
        if places[-1] - places[0] == 7:
            return [(places[0] * SLOT, (places[-1] + 1) * SLOT)]
        return [(places[i] * SLOT, (places[i + 3] + 1) * SLOT) for i in (0, 4)]

    own_slots = dot(spread[...], normed[tp]).astype(BF16)
    slots[pl.ds(0, PACKED)] = own_slots
    for chunk, ds in enumerate(CHUNKS):
        over_sp(slots, arrived, chunk, [-d for d in ds])

    tokens = jnp.concatenate([normed[i] for i in range(TP)], axis=1)
    both = dot_nt(tokens, shared_w[...])
    gate_part, up_part = both[:, :SHARED], both[:, SHARED:]
    units = gate_part * jax.nn.sigmoid(gate_part) * up_part
    shared[tp] = jnp.concatenate([units[: TOK // 2], units[TOK // 2 :]], axis=1).astype(BF16)
    gathers = {"g0": gather(1, shared, [32 * i for i in range(5)])}
    gathers["g0"].start()
    mine, mine_end = BACK * SLOT, (BACK + 1) * SLOT

    def rows_of(buf, own_rows, first_row, end):
        if not first_row <= mine < end:
            return [buf[pl.ds(first_row, end - first_row)]]
        return [
            buf[pl.ds(first_row, mine - first_row)],
            own_rows,
            buf[pl.ds(mine_end, end - mine_end)],
        ]

    def begin(chunk):
        over_sp_all(arrived, chunk).wait_recv()
        parts = [
            part
            for first_row, end in runs(chunk)
            for part in rows_of(arrived, own_slots[mine:mine_end], first_row, end)
        ]
        buf = (in0, in1, in2, in3)[chunk]
        buf[tp] = dot(squeeze[...], jnp.concatenate(parts, axis=0)).astype(BF16)
        gathers["i" + str(chunk)] = gather(2 + chunk, buf, CUTS[chunk % 2])
        gathers["i" + str(chunk)].start()

    def run_expert(chunk):
        rows_in, mid = (in0, in1, in2, in3)[chunk], (mid0, mid1, mid2, mid3)[chunk]
        u = jnp.concatenate([rows_in[j] for j in range(TP)], axis=1)
        both = dot(u, expert_w[...])
        gate_part = both[:, :LANES]
        mid[tp] = (gate_part * jax.nn.sigmoid(gate_part) * both[:, LANES:]).astype(BF16)
        gathers["h" + str(chunk)] = gather(6 + chunk, mid, CUTS[chunk % 2])
        gathers["h" + str(chunk)].start()

    def run_down(chunk):
        if chunk == 0:
            all_of(down_w, 1).wait_recv()
        mid = (mid0, mid1, mid2, mid3)[chunk]
        units = jnp.concatenate([mid[j] for j in range(TP)], axis=1)
        result = dot(units, down_w[...].reshape(D, LANES)).astype(BF16)
        result = dot(widen[...], result).astype(BF16)
        done = 0
        for first_row, end in runs(chunk):
            back[pl.ds(first_row, end - first_row)] = result[done : done + end - first_row]
            done += end - first_row
        over_sp(back, returned, 4 + chunk, CHUNKS[chunk])

    for op in [op for line in ORDER for op in line.split()]:
        if op[0] == "z":
            begin(int(op[1]))
        elif op[0] == "s":

            @pl.loop(1, TP)
            def _(d):
                source = sdown_hbm.at[:, pl.ds(pl.multiple_of(tp_at(d) * LANES, LANES), LANES)]
                remote(source, sdown_w.at[tp], t_send.at[2], t_recv.at[2], tp=tp_at(d)).start()

        else:
            gathers[op[:2]].stage(int(op[2]))
            if op[0] == "i" and op[2] == "5":
                run_expert(int(op[1]))
            elif op[0] == "h" and op[2] == "5":
                run_down(int(op[1]))

    all_of(sdown_w, 2).wait_recv()
    shared_units = jnp.concatenate([shared[i] for i in range(TP)], axis=1)
    nothing = jnp.zeros((SHARED, LANES), BF16)
    parts = [sdown_w[i] for i in range(TP)]
    low = jnp.concatenate([r for part in parts for r in (part, nothing)], axis=0)
    high = jnp.concatenate([r for part in parts for r in (nothing, part)], axis=0)
    shared_out = jnp.concatenate([dot(shared_units, low), dot(shared_units, high)], axis=0)
    base = RESIDUAL_SCALE * normed[tp].astype(F32) + shared_out

    for chunk in range(4):
        over_sp_all(returned, 4 + chunk).wait_recv()
    got = jnp.concatenate(rows_of(returned, back[pl.ds(mine, SLOT)], 0, PACKED), axis=0)
    second = base + (dot(picks_hi[...], got) + dot(picks_lo[...], got))

    lane = iota((TOK, LANES), 1)
    total = jnp.sum(second, axis=1, keepdims=True)
    squares = jnp.sum(second * second, axis=1, keepdims=True)
    both = jnp.where(lane == 0, total, jnp.where(lane == 1, squares, 0.0))
    stats[tp] = jnp.transpose(both)[:2]

    @pl.loop(1, TP)
    def _(d):
        to_all(stats, 3)(d).start()

    all_of(stats, 3).wait_recv()
    sums = stats[0]
    for i in range(1, TP):
        sums += stats[i]
    sums = jnp.transpose(jnp.concatenate([sums, jnp.zeros((6, TOK), F32)], axis=0))
    mean = sums[:, 0:1] / D
    var = sums[:, 1:2] / D - mean * mean
    settled = (second - mean) * lax.rsqrt(var + NORM_EPS)
    out[...] = (settled * gain2[...] + bias2[...]).astype(BF16)

    tail.wait_send()
    tail_docs.wait_send()
    for g in (g1, *gathers.values()):
        g.drain()
    for number, ref in enumerate((halo, down_w, sdown_w, stats)):
        all_of(ref, number).wait_send()
    for number in range(8):
        over_sp_all(slots if number < 4 else back, number).wait_send()


def shards(
    layer_input, doc_ids, routes, route_weight, pool_weight, pool_scale, norm1_gain, norm1_bias,
    expert_gate, expert_up, expert_down, shared_gate, shared_up, shared_down, norm2_gain, norm2_bias,
):
    vmem = pl.BlockSpec(memory_space=pltpu.VMEM)
    hbm = pl.BlockSpec(memory_space=pl.ANY)
    dma = pltpu.SemaphoreType.DMA
    scratch = [
        pltpu.VMEM((TP, TOK, LANES), BF16),
        pltpu.VMEM((TP, HALO, LANES), BF16),
        pltpu.VMEM((1, LANES), jnp.int32),
        pltpu.VMEM((4, TOK, GROUP), F32),
        pltpu.VMEM((TP, TOK, LANES), BF16),
        pltpu.VMEM((PADDED, LANES), BF16),
        pltpu.VMEM((PADDED, LANES), BF16),
        *[pltpu.VMEM((TP, HALF, LANES), BF16)] * 8,
        pltpu.VMEM((TP, TOK // 2, LANES), BF16),
        pltpu.VMEM((PADDED, LANES), BF16),
        pltpu.VMEM((PADDED, LANES), BF16),
        pltpu.VMEM((TP, 2, TOK), F32),
        pltpu.VMEM((4, GROUP, GROUP), BF16),
        pltpu.VMEM((D, 2 * LANES), BF16),
        pltpu.VMEM((2 * SHARED, D), BF16),
        pltpu.VMEM((TP, LANES, LANES), BF16),
        pltpu.VMEM((TP, SHARED, LANES), BF16),
        pltpu.VMEM((4, TOK, TOK), BF16),
        pltpu.VMEM((PACKED, TOK), BF16),
        pltpu.VMEM((TOK, PACKED), BF16),
        pltpu.VMEM((TOK, PACKED), BF16),
        pltpu.VMEM((HALF, WIDE), BF16),
        pltpu.VMEM((WIDE, HALF), BF16),
        dma((8,)),
    ]
    scratch += [dma((10,)), dma((10, 6)), dma((8,)), dma((8,)), dma((6,)), dma((6,))]
    return pl.pallas_call(
        layer,
        out_shape=jax.ShapeDtypeStruct((TOK, LANES), BF16),
        in_specs=[vmem] * 8 + [hbm] * 8,
        out_specs=vmem,
        scratch_shapes=scratch,
        compiler_params=pltpu.CompilerParams(
            collective_id=0, has_side_effects=True, vmem_limit_bytes=60 * 1024 * 1024
        ),
    )(
        doc_ids.reshape(1, TOK), routes.T, route_weight.T,
        pool_scale.reshape(1, D), norm1_gain.reshape(1, D), norm1_bias.reshape(1, D),
        norm2_gain.reshape(1, LANES), norm2_bias.reshape(1, LANES),
        layer_input, pool_weight, expert_gate, expert_up, expert_down,
        shared_gate.T, shared_up.T, shared_down,
    )


def solution(mesh):
    placed = (
        P("sp", "tp"), P("sp"), P("sp", None), P("sp", None), P(), P(), P(), P(),
        P("sp", None, "tp"), P("sp", None, "tp"), P("sp", "tp", None),
        P(None, "tp"), P(None, "tp"), P("tp", None), P("tp"), P("tp"),
    )
    return jax.shard_map(
        shards, mesh=mesh, in_specs=placed, out_specs=P("sp", "tp"), check_vma=False
    )
```

```python
import functools

import jax
import jax.numpy as jnp
from jax import lax
from jax.experimental import pallas as pl
from jax.experimental.pallas import tpu as pltpu
from jax.sharding import PartitionSpec as P

MESH = pl.DeviceIdType.MESH
WINDOWS = (2, 4, 8, 16)
RESIDUAL_SCALE = 2.0**0.5
NORM_EPS = 1e-05

SP = 32
TP = 16
TOK = 256
LANES = 128
D = 2048
GROUP = 512
HALO = 16
SHARED = 64
CAP = 22
SLOT = 24
PACKED = SP * SLOT
PADDED = PACKED + 8
BACK = 8
UNITS = (
    tuple(range(-8, 0)),
    tuple(range(0, 8)),
    tuple(range(8, 12)) + tuple(range(-12, -8)),
    tuple(range(12, 20)),
)
CHUNKS = ((0, 1), (2,), (3,))
ROWS = 8 * CAP
WIDE = 8 * SLOT
CUTS = (ROWS, 96, 80)
ORDER = (
    "g00 g01 z0 i00",
    "z1 i01 z2 i10",
    "i11 i20 i21 i02",
    "i12 i22 g02 h10",
    "h11 h20 h21 h00",
    "h01 s0 h12",
    "h22 h02",
)

F32 = jnp.float32
BF16 = jnp.bfloat16


def iota(shape, dim):
    return lax.broadcasted_iota(jnp.int32, shape, dim)


def dot(a, b):
    return jnp.dot(a, b, preferred_element_type=F32)


def dot_nt(a, b):
    return lax.dot_general(a, b, (((1,), (1,)), ((), ())), preferred_element_type=F32)


class Gather:
    def __init__(self, buf, cut, tp, send_sem, recv_sem):
        self.buf, self.tp = buf, tp
        self.rows = (pl.ds(0, cut), pl.ds(cut, buf.shape[1] - cut))
        self.send_sem, self.recv_sem = send_sem, recv_sem

    def at(self, colour, a, b):
        y, x = self.tp // 4, lax.rem(self.tp, 4)
        dx, dy = (a, b) if colour == 0 else (b, a)
        return lax.rem(y + dy + 4, 4) * 4 + lax.rem(x + dx + 4, 4)

    def copy(self, ref, number, to):
        return pltpu.make_async_remote_copy(
            src_ref=ref,
            dst_ref=ref,
            send_sem=self.send_sem.at[0],
            recv_sem=self.recv_sem.at[number],
            device_id={"tp": to},
            device_id_type=MESH,
        )

    def send(self, number, colour, block, to):
        self.copy(self.buf.at[block, self.rows[colour]], number, to).start()

    def onward(self, *sources):
        for b in (1, -1, 2):
            for a in sources:
                for c in (0, 1):
                    self.send(2, c, self.at(c, a, 0), self.at(c, 0, b))

    def start(self):
        for number, ways in ((0, (1, -1)), (1, (2,))):
            for a in ways:
                for c in (0, 1):
                    self.send(number, c, self.tp, self.at(c, a, 0))
        self.onward(0)

    def stage(self, number):
        self.copy(self.buf.at[pl.ds(0, (2, 1, 12)[number])], number, self.at(0, 1, 0)).wait_recv()
        if number == 0:
            self.onward(-1, 1)
        elif number == 1:
            self.onward(2)

    def drain(self):
        self.copy(self.buf.at[pl.ds(0, 15)], 0, self.at(0, 1, 0)).wait_send()


def layer(
    docs_hbm, routes_hbm, weights_hbm, scale_hbm, gain1_hbm, bias1_hbm, gain2_hbm, bias2_hbm,
    x_hbm, pool_hbm, gate_hbm, up_hbm, down_hbm, sgate_hbm, sup_hbm, sdown_hbm,
    out,
    docs, routes, weights, scale, gain1, bias1, gain2, bias2,
    x_buf, halo, halo_docs, first, normed, slots, arrived,
    in0, in1, in2, mid0, mid1, mid2, shared, back, returned, stats,
    pool_w, expert_w, shared_w, down_w, sdown_w,
    bands, spread, picks_hi, picks_lo, squeeze, widen,
    load_sem, g_send, g_recv, z_send, z_recv, t_send, t_recv,
):
    sp, tp = lax.axis_index("sp"), lax.axis_index("tp")

    def sp_at(d):
        return lax.rem(sp + d + SP, SP)

    def tp_at(d):
        return lax.rem(tp + d, TP)

    barrier = pltpu.get_barrier_semaphore()

    def greet_sp(d):
        pl.semaphore_signal(barrier, 1, device_id={"sp": sp_at(d)}, device_id_type=MESH)

    pl.loop(9, 24)(greet_sp)

    @pl.loop(1, TP)
    def _(d):
        pl.semaphore_signal(barrier, 1, device_id={"tp": tp_at(d)}, device_id_type=MESH)

    pl.loop(1, 9)(greet_sp)
    pl.loop(24, SP)(greet_sp)

    loads = [
        (docs_hbm, docs), (routes_hbm, routes), (weights_hbm, weights),
        (x_hbm, x_buf.at[tp]),
        (pool_hbm, pool_w),
        (gate_hbm.at[0], expert_w.at[:, pl.ds(0, LANES)]),
        (up_hbm.at[0], expert_w.at[:, pl.ds(LANES, LANES)]),
        (sgate_hbm, shared_w.at[pl.ds(0, SHARED)]),
        (sup_hbm, shared_w.at[pl.ds(SHARED, SHARED)]),
        (down_hbm.at[0, :, pl.ds(pl.multiple_of(tp * LANES, LANES), LANES)], down_w.at[tp]),
        (sdown_hbm.at[:, pl.ds(pl.multiple_of(tp * LANES, LANES), LANES)], sdown_w.at[tp]),
        (scale_hbm, scale), (gain1_hbm, gain1), (bias1_hbm, bias1), (gain2_hbm, gain2), (bias2_hbm, bias2),
    ]
    loads = [pltpu.make_async_copy(s, d, load_sem.at[i]) for i, (s, d) in enumerate(loads)]
    for load in loads:
        load.start()

    for load in loads[:3]:
        load.wait()

    route_rows = routes[...]
    expert = iota((SP, TOK), 0)
    names = [(route_rows[k : k + 1] == expert).astype(F32) for k in (0, 1)]
    before = (iota((TOK, TOK), 0) < iota((TOK, TOK), 1)).astype(F32).astype(BF16)
    rank = dot((names[0] + names[1]).astype(BF16), before)
    order = jnp.bitwise_and(expert - sp + (SP + BACK), SP - 1)
    place = order.astype(F32) * SLOT + rank
    places = [jnp.sum(n * place, axis=0, keepdims=True) for n in names]
    row = iota((PACKED, TOK), 0).astype(F32)
    spread[...] = ((row == places[0]) | (row == places[1])).astype(F32).astype(BF16)
    rows8 = jnp.concatenate(places + [weights[...], jnp.zeros((4, TOK), F32)], axis=0)
    cols = jnp.transpose(rows8)
    column = iota((TOK, PACKED), 1).astype(F32)
    picks = jnp.where(column == cols[:, 0:1], cols[:, 2:3], 0.0)
    picks += jnp.where(column == cols[:, 1:2], cols[:, 3:4], 0.0)
    high = picks.astype(BF16)
    picks_hi[...] = high
    picks_lo[...] = (picks - high.astype(F32)).astype(BF16)

    tight = iota((2 * ROWS, 1), 0).astype(F32)
    tight = tight + 2.0 * jnp.floor((tight + 0.5) * (1.0 / CAP))
    squeeze[...] = (iota((2 * ROWS, 2 * WIDE), 1).astype(F32) == tight).astype(F32).astype(BF16)
    tight = iota((1, ROWS), 1).astype(F32)
    tight = tight + 2.0 * jnp.floor((tight + 0.5) * (1.0 / CAP))
    widen[...] = (iota((WIDE, ROWS), 0).astype(F32) == tight).astype(F32).astype(BF16)

    marks_row = docs[...].astype(F32)
    p, q = iota((TOK, TOK), 0), iota((TOK, TOK), 1)
    marks_col = jnp.sum(jnp.where(p == q, marks_row, 0.0), axis=1, keepdims=True)
    same = (marks_row == marks_col) & (q <= p)
    members = []
    for g, window in enumerate(WINDOWS):
        band = (same & (q > p - window)).astype(F32)
        bands[g] = band.astype(BF16)
        members.append(jnp.sum(band, axis=1, keepdims=True))

    loads[3].wait()
    pl.semaphore_wait(barrier, SP - 1 + TP - 1)

    def remote(src, dst, send_sem, recv_sem, **to):
        return pltpu.make_async_remote_copy(
            src_ref=src, dst_ref=dst, send_sem=send_sem, recv_sem=recv_sem,
            device_id=to, device_id_type=MESH,
        )

    def to_all(ref, number):
        def copy(d):
            return remote(ref.at[tp], ref.at[tp], t_send.at[number], t_recv.at[number], tp=tp_at(d))

        return copy

    def all_of(ref, number):
        block = ref.at[pl.ds(0, TP - 1)]
        return remote(block, block, t_send.at[number], t_recv.at[number], tp=tp_at(1))

    tail = remote(
        x_buf.at[tp, pl.ds(TOK - HALO, HALO)], halo.at[tp], t_send.at[4], t_recv.at[4], sp=sp_at(1)
    )
    tail_docs = remote(docs.at[:, pl.ds(LANES, LANES)], halo_docs, t_send.at[5], t_recv.at[5], sp=sp_at(1))
    tail.start()
    tail_docs.start()
    def gather(number, buf, cut):
        return Gather(buf, cut, tp, g_send.at[pl.ds(number, 1)], g_recv.at[number])

    g1 = gather(0, x_buf, TOK // 2)
    g1.start()
    tail.wait_recv()

    @pl.loop(1, TP)
    def _(d):
        to_all(halo, 0)(d).start()

    tail_docs.wait_recv()
    halo_marks = halo_docs[...][:, LANES - HALO :].astype(F32)
    hp, hq = iota((HALO, HALO), 0), iota((HALO, HALO), 1) - HALO
    halo_same = (halo_marks == marks_col[:HALO]) & (sp > 0)
    g1.stage(0)
    g1.stage(1)

    def columns(d):
        return pl.ds(pl.multiple_of(tp_at(d) * LANES, LANES), LANES)

    @pl.loop(1, TP)
    def _(d):
        source = down_hbm.at[0, :, columns(d)]
        remote(source, down_w.at[tp], t_send.at[1], t_recv.at[1], tp=tp_at(d)).start()

    g1.stage(2)

    for load in loads[4:]:
        load.wait()
    all_of(halo, 0).wait_recv()

    total = jnp.zeros((TOK, 1), F32)
    squares = jnp.zeros((TOK, 1), F32)
    for g, window in enumerate(WINDOWS):
        halo_band = (halo_same & (hq > hp - window)).astype(F32)
        halo_members = members[g][:HALO] + jnp.sum(halo_band, axis=1, keepdims=True)
        share = 1.0 / jnp.concatenate([halo_members, members[g][HALO:]], axis=0)
        values = jnp.concatenate([x_buf[4 * g + i] for i in range(4)], axis=1)
        halo_values = jnp.concatenate([halo[4 * g + i] for i in range(4)], axis=1)
        running = dot(bands[g], values)
        halo_running = running[:HALO] + dot(halo_band.astype(BF16), halo_values)
        running = jnp.concatenate([halo_running, running[HALO:]], axis=0)
        mixed = (running * share - values.astype(F32)).astype(BF16)
        here = pl.ds(g * GROUP, GROUP)
        projected = dot(mixed, pool_w[g]) * scale[:, here]
        value = RESIDUAL_SCALE * values.astype(F32) + projected
        first[g] = value
        total += jnp.sum(value, axis=1, keepdims=True)
        squares += jnp.sum(value * value, axis=1, keepdims=True)
    mean = total / D
    factor = lax.rsqrt(squares / D - mean * mean + NORM_EPS)
    for g in range(4):
        here = pl.ds(g * GROUP, GROUP)
        value = ((first[g] - mean) * factor * gain1[:, here] + bias1[:, here]).astype(BF16)
        for i in range(4):
            normed[4 * g + i] = value[:, i * LANES : (i + 1) * LANES]

    def block(d):
        return pl.ds((d + BACK) % SP * SLOT, SLOT)

    def over_sp(source, target, number, ds):
        for d in ds:
            if d != 0:
                remote(
                    source.at[block(d)], target.at[block(-d)],
                    z_send.at[number], z_recv.at[number], sp=sp_at(d),
                ).start()

    def over_sp_all(ref, number, blocks):
        rows = ref.at[pl.ds(0, blocks * SLOT)]
        return remote(rows, rows, z_send.at[number], z_recv.at[number], sp=sp_at(1))

    def runs(unit):
        places = [(d + BACK) % SP for d in UNITS[unit]]
        if places[-1] - places[0] == 7:
            return [(places[0] * SLOT, (places[-1] + 1) * SLOT)]
        return [(places[i] * SLOT, (places[i + 3] + 1) * SLOT) for i in (0, 4)]

    near = 18 * SLOT
    own_slots = dot(spread[pl.ds(0, near)], normed[tp]).astype(BF16)
    slots[pl.ds(0, near)] = own_slots
    over_sp(slots, arrived, 0, [-d for unit in CHUNKS[0] for d in UNITS[unit]])
    rest = pl.ds(near, PACKED - near)
    slots[rest] = dot(spread[rest], normed[tp]).astype(BF16)
    for chunk in (1, 2):
        over_sp(slots, arrived, chunk, [-d for d in UNITS[chunk + 1]])

    tokens = jnp.concatenate([normed[i] for i in range(TP)], axis=1)
    both = dot_nt(tokens, shared_w[...])
    gate_part, up_part = both[:, :SHARED], both[:, SHARED:]
    units = gate_part * jax.nn.sigmoid(gate_part) * up_part
    shared[tp] = jnp.concatenate([units[: TOK // 2], units[TOK // 2 :]], axis=1).astype(BF16)
    gathers = {"g0": gather(1, shared, TOK // 4)}
    gathers["g0"].start()
    mine, mine_end = BACK * SLOT, (BACK + 1) * SLOT
    ins, mids = (in0, in1, in2), (mid0, mid1, mid2)

    def rows_of(buf, own_rows, first_row, end):
        parts = [(first_row, mine), (mine, mine_end), (mine_end, end)]
        if not first_row <= mine < end:
            parts = [(first_row, end)]
        parts = [(lo, hi) for lo, hi in parts if lo < hi]
        return [own_rows if lo == mine else buf[pl.ds(lo, hi - lo)] for lo, hi in parts]

    def begin(chunk):
        over_sp_all(arrived, chunk, 15 if chunk == 0 else 8).wait_recv()
        parts = [
            part
            for unit in CHUNKS[chunk]
            for first_row, end in runs(unit)
            for part in rows_of(arrived, own_slots[mine:mine_end], first_row, end)
        ]
        count = len(CHUNKS[chunk])
        tight = squeeze[pl.ds(0, count * ROWS), pl.ds(0, count * WIDE)]
        ins[chunk][tp] = dot(tight, jnp.concatenate(parts, axis=0)).astype(BF16)
        gathers["i" + str(chunk)] = gather(2 + chunk, ins[chunk], CUTS[chunk])
        gathers["i" + str(chunk)].start()

    def run_expert(chunk):
        for i in range(len(CHUNKS[chunk])):
            rows = pl.ds(i * ROWS, ROWS)
            u = jnp.concatenate([ins[chunk][j, rows] for j in range(TP)], axis=1)
            both = dot(u, expert_w[...])
            gate_part = both[:, :LANES]
            value = gate_part * jax.nn.sigmoid(gate_part) * both[:, LANES:]
            mids[chunk][tp, rows] = value.astype(BF16)
        gathers["h" + str(chunk)] = gather(5 + chunk, mids[chunk], CUTS[chunk])
        gathers["h" + str(chunk)].start()

    def run_down(chunk):
        if chunk == 1:
            all_of(down_w, 1).wait_recv()
        for i, unit in enumerate(CHUNKS[chunk]):
            units = [mids[chunk][j, pl.ds(i * ROWS, ROWS)] for j in range(TP)]
            result = dot(jnp.concatenate(units, axis=1), down_w[...].reshape(D, LANES))
            result = dot(widen[...], result.astype(BF16)).astype(BF16)
            done = 0
            for first_row, end in runs(unit):
                back[pl.ds(first_row, end - first_row)] = result[done : done + end - first_row]
                done += end - first_row
            over_sp(back, returned, 3 + unit, UNITS[unit])

    for op in [op for line in ORDER for op in line.split()]:
        if op[0] == "z":
            begin(int(op[1]))
        elif op[0] == "s":

            @pl.loop(1, TP)
            def _(d):
                source = sdown_hbm.at[:, columns(d)]
                remote(source, sdown_w.at[tp], t_send.at[2], t_recv.at[2], tp=tp_at(d)).start()

        else:
            gathers[op[:2]].stage(int(op[2]))
            if op[0] == "i" and op[2] == "2":
                run_expert(int(op[1]))
            elif op[0] == "h" and op[2] == "2":
                run_down(int(op[1]))

    all_of(sdown_w, 2).wait_recv()
    shared_units = jnp.concatenate([shared[i] for i in range(TP)], axis=1)
    nothing = jnp.zeros((SHARED, LANES), BF16)
    parts = [sdown_w[i] for i in range(TP)]
    low = jnp.concatenate([r for part in parts for r in (part, nothing)], axis=0)
    high = jnp.concatenate([r for part in parts for r in (nothing, part)], axis=0)
    shared_out = jnp.concatenate([dot(shared_units, low), dot(shared_units, high)], axis=0)
    base = RESIDUAL_SCALE * normed[tp].astype(F32) + shared_out

    for unit in (2, 3, 0, 1):
        over_sp_all(returned, 3 + unit, 7 if unit == 1 else 8).wait_recv()
    got = jnp.concatenate(rows_of(returned, back[pl.ds(mine, SLOT)], 0, PACKED), axis=0)
    second = base + (dot(picks_hi[...], got) + dot(picks_lo[...], got))

    lane = iota((TOK, LANES), 1)
    total = jnp.sum(second, axis=1, keepdims=True)
    squares = jnp.sum(second * second, axis=1, keepdims=True)
    both = jnp.where(lane == 0, total, jnp.where(lane == 1, squares, 0.0))
    stats[tp] = jnp.transpose(both)[:2]

    @pl.loop(1, TP)
    def _(d):
        to_all(stats, 3)(d).start()

    all_of(stats, 3).wait_recv()
    sums = stats[0]
    for i in range(1, TP):
        sums += stats[i]
    sums = jnp.transpose(jnp.concatenate([sums, jnp.zeros((6, TOK), F32)], axis=0))
    mean = sums[:, 0:1] / D
    var = sums[:, 1:2] / D - mean * mean
    settled = (second - mean) * lax.rsqrt(var + NORM_EPS)
    out[...] = (settled * gain2[...] + bias2[...]).astype(BF16)

    tail.wait_send()
    tail_docs.wait_send()
    for g in (g1, *gathers.values()):
        g.drain()
    for number, ref in enumerate((halo, down_w, sdown_w, stats)):
        all_of(ref, number).wait_send()
    for number, blocks in enumerate((15, 8, 8, 8, 7, 8, 8)):
        over_sp_all(slots if number < 3 else back, number, blocks).wait_send()


def shards(
    layer_input, doc_ids, routes, route_weight, pool_weight, pool_scale, norm1_gain, norm1_bias,
    expert_gate, expert_up, expert_down, shared_gate, shared_up, shared_down, norm2_gain, norm2_bias,
):
    vmem = pl.BlockSpec(memory_space=pltpu.VMEM)
    hbm = pl.BlockSpec(memory_space=pl.ANY)
    dma = pltpu.SemaphoreType.DMA
    scratch = [
        pltpu.VMEM((1, TOK), jnp.int32),
        pltpu.VMEM((2, TOK), jnp.int32),
        pltpu.VMEM((2, TOK), F32),
        *[pltpu.VMEM((1, D), F32)] * 3,
        *[pltpu.VMEM((1, LANES), F32)] * 2,
        pltpu.VMEM((TP, TOK, LANES), BF16),
        pltpu.VMEM((TP, HALO, LANES), BF16),
        pltpu.VMEM((1, LANES), jnp.int32),
        pltpu.VMEM((4, TOK, GROUP), F32),
        pltpu.VMEM((TP, TOK, LANES), BF16),
        pltpu.VMEM((PADDED, LANES), BF16),
        pltpu.VMEM((PADDED, LANES), BF16),
        *[pltpu.VMEM((TP, n * ROWS, LANES), BF16) for n in (2, 1, 1) * 2],
        pltpu.VMEM((TP, TOK // 2, LANES), BF16),
        pltpu.VMEM((PADDED, LANES), BF16),
        pltpu.VMEM((PADDED, LANES), BF16),
        pltpu.VMEM((TP, 2, TOK), F32),
        pltpu.VMEM((4, GROUP, GROUP), BF16),
        pltpu.VMEM((D, 2 * LANES), BF16),
        pltpu.VMEM((2 * SHARED, D), BF16),
        pltpu.VMEM((TP, LANES, LANES), BF16),
        pltpu.VMEM((TP, SHARED, LANES), BF16),
        pltpu.VMEM((4, TOK, TOK), BF16),
        pltpu.VMEM((PACKED, TOK), BF16),
        pltpu.VMEM((TOK, PACKED), BF16),
        pltpu.VMEM((TOK, PACKED), BF16),
        pltpu.VMEM((2 * ROWS, 2 * WIDE), BF16),
        pltpu.VMEM((WIDE, ROWS), BF16),
        dma((16,)),
    ]
    scratch += [dma((8,)), dma((8, 3)), dma((7,)), dma((7,)), dma((6,)), dma((6,))]
    return pl.pallas_call(
        layer,
        out_shape=jax.ShapeDtypeStruct((TOK, LANES), BF16),
        in_specs=[hbm] * 16,
        out_specs=vmem,
        scratch_shapes=scratch,
        compiler_params=pltpu.CompilerParams(
            collective_id=0, has_side_effects=True, vmem_limit_bytes=60 * 1024 * 1024
        ),
    )(
        doc_ids.reshape(1, TOK), routes.T, route_weight.T,
        pool_scale.reshape(1, D), norm1_gain.reshape(1, D), norm1_bias.reshape(1, D),
        norm2_gain.reshape(1, LANES), norm2_bias.reshape(1, LANES),
        layer_input, pool_weight, expert_gate, expert_up, expert_down,
        shared_gate.T, shared_up.T, shared_down,
    )


def solution(mesh):
    placed = (
        P("sp", "tp"), P("sp"), P("sp", None), P("sp", None), P(), P(), P(), P(),
        P("sp", None, "tp"), P("sp", None, "tp"), P("sp", "tp", None),
        P(None, "tp"), P(None, "tp"), P("tp", None), P("tp"), P("tp"),
    )
    return jax.shard_map(
        shards, mesh=mesh, in_specs=placed, out_specs=P("sp", "tp"), check_vma=False
    )
```

```python
import functools

import jax
import jax.numpy as jnp
from jax import lax
from jax.experimental import pallas as pl
from jax.experimental.pallas import tpu as pltpu
from jax.sharding import PartitionSpec as P

MESH = pl.DeviceIdType.MESH
WINDOWS = (2, 4, 8, 16)
RESIDUAL_SCALE = 2.0**0.5
NORM_EPS = 1e-05

SP = 32
TP = 16
TOK = 256
LANES = 128
D = 2048
GROUP = 512
HALO = 16
SHARED = 64
CAP = 22
SLOT = 24
PACKED = SP * SLOT
PADDED = PACKED + 8
BACK = 8
UNITS = (
    tuple(range(-8, 0)),
    tuple(range(0, 8)),
    tuple(range(8, 12)) + tuple(range(-12, -8)),
    tuple(range(12, 20)),
)
CHUNKS = ((0, 1), (2,), (3,))
ROWS = 8 * CAP
WIDE = 8 * SLOT
CUTS = ((96, 176, 272), (48, 96, 144), (48, 80, 128))
ORDER = (
    "g00 g02 s0 z0",
    "z1 i00 i01 i02",
    "i10 i11 i12 z2",
    "i03 i13 i04 i14",
    "i20 i21 i22 i05",
    "i23 i24 i15 i25",
    "h10 h12 h20 h22",
    "g05 h00 h15 h02",
    "h25 h05",
)

F32 = jnp.float32
BF16 = jnp.bfloat16


def iota(shape, dim):
    return lax.broadcasted_iota(jnp.int32, shape, dim)


def dot(a, b):
    return jnp.dot(a, b, preferred_element_type=F32)


def dot_nt(a, b):
    return lax.dot_general(a, b, (((1,), (1,)), ((), ())), preferred_element_type=F32)


class Gather:
    def __init__(self, buf, cuts, tp, send_sem, recv_sem, relay=False):
        self.buf, self.tp, self.relay = buf, tp, relay
        c0, c1, c2 = cuts
        end = buf.shape[1]
        whole = (pl.ds(0, c1), pl.ds(c1, end - c1))
        low = (pl.ds(0, c0), pl.ds(c1, c2 - c1))
        high = (pl.ds(c0, c1 - c0), pl.ds(c2, end - c2))
        self.parts = {"all": whole, "lo": low, "hi": high}
        self.send_sem, self.recv_sem = send_sem, recv_sem

    def at(self, colour, a, b):
        y, x = self.tp // 4, lax.rem(self.tp, 4)
        dx, dy = (a, b) if colour == 0 else (b, a)
        return lax.rem(y + dy + 4, 4) * 4 + lax.rem(x + dx + 4, 4)

    def copy(self, ref, number, to):
        return pltpu.make_async_remote_copy(
            src_ref=ref,
            dst_ref=ref,
            send_sem=self.send_sem.at[0],
            recv_sem=self.recv_sem.at[number],
            device_id={"tp": to},
            device_id_type=MESH,
        )

    def send(self, number, colour, block, to, part="all"):
        self.copy(self.buf.at[block, self.parts[part][colour]], number, to).start()

    def onward(self, number, *sources):
        for b in (1, -1) if self.relay else (1, -1, 2):
            for a in sources:
                for c in (0, 1):
                    where = number if self.relay else 5
                    self.send(where, c, self.at(c, a, 0), self.at(c, 0, b))

    def opposite(self, *sources):
        for way, part in ((1, "lo"), (-1, "hi")):
            for a in sources:
                for c in (0, 1):
                    self.send(5, c, self.at(c, a, -way), self.at(c, 0, way), part)

    def start(self):
        for number, ways in ((0, (1, -1)), (2, (2,))):
            for a in ways:
                for c in (0, 1):
                    self.send(number, c, self.tp, self.at(c, a, 0))
        self.onward(1, 0)

    def stage(self, number):
        blocks = (2, 2, 1, 4, 2, 4 if self.relay else 12)[number]
        self.copy(self.buf.at[pl.ds(0, blocks)], number, self.at(0, 1, 0)).wait_recv()
        if number == 0:
            self.onward(3, -1, 1)
        elif number == 1:
            self.opposite(0)
        elif number == 2:
            self.onward(4, 2)
        elif number == 3:
            self.opposite(-1, 1)
        elif number == 4:
            self.opposite(2)

    def drain(self):
        self.copy(self.buf.at[pl.ds(0, 15)], 0, self.at(0, 1, 0)).wait_send()


def layer(
    docs_hbm, routes_hbm, weights_hbm, scale_hbm, gain1_hbm, bias1_hbm, gain2_hbm, bias2_hbm,
    x_hbm, pool_hbm, gate_hbm, up_hbm, down_hbm, sgate_hbm, sup_hbm, sdown_hbm,
    out,
    docs, routes, weights, scale, gain1, bias1, gain2, bias2,
    x_buf, halo, halo_docs, first, normed, slots, arrived,
    in0, in1, in2, mid0, mid1, mid2, shared, back, returned, stats,
    pool_w, expert_w, shared_w, down_w, sdown_w,
    bands, spread, picks_hi, picks_lo, squeeze, widen,
    load_sem, g_send, g_recv, z_send, z_recv, t_send, t_recv,
):
    sp, tp = lax.axis_index("sp"), lax.axis_index("tp")

    def sp_at(d):
        return lax.rem(sp + d + SP, SP)

    def tp_at(d):
        return lax.rem(tp + d, TP)

    barrier = pltpu.get_barrier_semaphore()

    def greet_sp(d):
        pl.semaphore_signal(barrier, 1, device_id={"sp": sp_at(d)}, device_id_type=MESH)

    pl.loop(9, 24)(greet_sp)

    @pl.loop(1, TP)
    def _(d):
        pl.semaphore_signal(barrier, 1, device_id={"tp": tp_at(d)}, device_id_type=MESH)

    pl.loop(1, 9)(greet_sp)
    pl.loop(24, SP)(greet_sp)

    loads = [
        (docs_hbm, docs), (routes_hbm, routes), (weights_hbm, weights),
        (x_hbm, x_buf.at[tp]),
        (pool_hbm, pool_w),
        (gate_hbm.at[0], expert_w.at[:, pl.ds(0, LANES)]),
        (up_hbm.at[0], expert_w.at[:, pl.ds(LANES, LANES)]),
        (sgate_hbm, shared_w.at[pl.ds(0, SHARED)]),
        (sup_hbm, shared_w.at[pl.ds(SHARED, SHARED)]),
        (down_hbm.at[0, :, pl.ds(pl.multiple_of(tp * LANES, LANES), LANES)], down_w.at[tp]),
        (sdown_hbm.at[:, pl.ds(pl.multiple_of(tp * LANES, LANES), LANES)], sdown_w.at[tp]),
        (scale_hbm, scale), (gain1_hbm, gain1), (bias1_hbm, bias1), (gain2_hbm, gain2), (bias2_hbm, bias2),
    ]
    loads = [pltpu.make_async_copy(s, d, load_sem.at[i]) for i, (s, d) in enumerate(loads)]
    for load in loads:
        load.start()

    for load in loads[:3]:
        load.wait()

    route_rows = routes[...]
    expert = iota((SP, TOK), 0)
    names = [(route_rows[k : k + 1] == expert).astype(F32) for k in (0, 1)]
    before = (iota((TOK, TOK), 0) < iota((TOK, TOK), 1)).astype(F32).astype(BF16)
    rank = dot((names[0] + names[1]).astype(BF16), before)
    order = jnp.bitwise_and(expert - sp + (SP + BACK), SP - 1)
    place = order.astype(F32) * SLOT + rank
    places = [jnp.sum(n * place, axis=0, keepdims=True) for n in names]
    row = iota((PACKED, TOK), 0).astype(F32)
    spread[...] = ((row == places[0]) | (row == places[1])).astype(F32).astype(BF16)
    rows8 = jnp.concatenate(places + [weights[...], jnp.zeros((4, TOK), F32)], axis=0)
    cols = jnp.transpose(rows8)
    column = iota((TOK, PACKED), 1).astype(F32)
    picks = jnp.where(column == cols[:, 0:1], cols[:, 2:3], 0.0)
    picks += jnp.where(column == cols[:, 1:2], cols[:, 3:4], 0.0)
    high = picks.astype(BF16)
    picks_hi[...] = high
    picks_lo[...] = (picks - high.astype(F32)).astype(BF16)

    tight = iota((2 * ROWS, 1), 0).astype(F32)
    tight = tight + 2.0 * jnp.floor((tight + 0.5) * (1.0 / CAP))
    squeeze[...] = (iota((2 * ROWS, 2 * WIDE), 1).astype(F32) == tight).astype(F32).astype(BF16)
    tight = iota((1, ROWS), 1).astype(F32)
    tight = tight + 2.0 * jnp.floor((tight + 0.5) * (1.0 / CAP))
    widen[...] = (iota((WIDE, ROWS), 0).astype(F32) == tight).astype(F32).astype(BF16)

    marks_row = docs[...].astype(F32)
    p, q = iota((TOK, TOK), 0), iota((TOK, TOK), 1)
    marks_col = jnp.sum(jnp.where(p == q, marks_row, 0.0), axis=1, keepdims=True)
    same = (marks_row == marks_col) & (q <= p)
    members = []
    for g, window in enumerate(WINDOWS):
        band = (same & (q > p - window)).astype(F32)
        bands[g] = band.astype(BF16)
        members.append(jnp.sum(band, axis=1, keepdims=True))

    loads[3].wait()
    pl.semaphore_wait(barrier, SP - 1 + TP - 1)

    def remote(src, dst, send_sem, recv_sem, **to):
        return pltpu.make_async_remote_copy(
            src_ref=src, dst_ref=dst, send_sem=send_sem, recv_sem=recv_sem,
            device_id=to, device_id_type=MESH,
        )

    def to_all(ref, number):
        def copy(d):
            return remote(ref.at[tp], ref.at[tp], t_send.at[number], t_recv.at[number], tp=tp_at(d))

        return copy

    def all_of(ref, number):
        block = ref.at[pl.ds(0, TP - 1)]
        return remote(block, block, t_send.at[number], t_recv.at[number], tp=tp_at(1))

    tail = remote(
        x_buf.at[tp, pl.ds(TOK - HALO, HALO)], halo.at[tp], t_send.at[4], t_recv.at[4], sp=sp_at(1)
    )
    tail_docs = remote(docs.at[:, pl.ds(LANES, LANES)], halo_docs, t_send.at[5], t_recv.at[5], sp=sp_at(1))
    tail.start()
    tail_docs.start()
    def gather(number, buf, cuts, relay=False):
        return Gather(buf, cuts, tp, g_send.at[pl.ds(number, 1)], g_recv.at[number], relay)

    g1 = gather(0, x_buf, (64, 128, 192))
    g1.start()
    tail.wait_recv()

    @pl.loop(1, TP)
    def _(d):
        to_all(halo, 0)(d).start()

    tail_docs.wait_recv()
    halo_marks = halo_docs[...][:, LANES - HALO :].astype(F32)
    hp, hq = iota((HALO, HALO), 0), iota((HALO, HALO), 1) - HALO
    halo_same = (halo_marks == marks_col[:HALO]) & (sp > 0)
    g1.stage(0)
    g1.stage(2)

    g1.stage(5)

    def columns(d):
        return pl.ds(pl.multiple_of(tp_at(d) * LANES, LANES), LANES)

    @pl.loop(1, TP)
    def _(d):
        source = down_hbm.at[0, :, columns(d)]
        remote(source, down_w.at[tp], t_send.at[1], t_recv.at[1], tp=tp_at(d)).start()

    for load in loads[4:]:
        load.wait()
    all_of(halo, 0).wait_recv()

    total = jnp.zeros((TOK, 1), F32)
    squares = jnp.zeros((TOK, 1), F32)
    for g, window in enumerate(WINDOWS):
        halo_band = (halo_same & (hq > hp - window)).astype(F32)
        halo_members = members[g][:HALO] + jnp.sum(halo_band, axis=1, keepdims=True)
        share = 1.0 / jnp.concatenate([halo_members, members[g][HALO:]], axis=0)
        values = jnp.concatenate([x_buf[4 * g + i] for i in range(4)], axis=1)
        halo_values = jnp.concatenate([halo[4 * g + i] for i in range(4)], axis=1)
        running = dot(bands[g], values)
        halo_running = running[:HALO] + dot(halo_band.astype(BF16), halo_values)
        running = jnp.concatenate([halo_running, running[HALO:]], axis=0)
        mixed = (running * share - values.astype(F32)).astype(BF16)
        here = pl.ds(g * GROUP, GROUP)
        projected = dot(mixed, pool_w[g]) * scale[:, here]
        value = RESIDUAL_SCALE * values.astype(F32) + projected
        first[g] = value
        total += jnp.sum(value, axis=1, keepdims=True)
        squares += jnp.sum(value * value, axis=1, keepdims=True)
    mean = total / D
    factor = lax.rsqrt(squares / D - mean * mean + NORM_EPS)
    for g in range(4):
        here = pl.ds(g * GROUP, GROUP)
        value = ((first[g] - mean) * factor * gain1[:, here] + bias1[:, here]).astype(BF16)
        for i in range(4):
            normed[4 * g + i] = value[:, i * LANES : (i + 1) * LANES]

    def block(d):
        return pl.ds((d + BACK) % SP * SLOT, SLOT)

    def over_sp(source, target, number, ds):
        for d in ds:
            if d != 0:
                remote(
                    source.at[block(d)], target.at[block(-d)],
                    z_send.at[number], z_recv.at[number], sp=sp_at(d),
                ).start()

    def over_sp_all(ref, number, blocks):
        rows = ref.at[pl.ds(0, blocks * SLOT)]
        return remote(rows, rows, z_send.at[number], z_recv.at[number], sp=sp_at(1))

    def runs(unit):
        places = [(d + BACK) % SP for d in UNITS[unit]]
        if places[-1] - places[0] == 7:
            return [(places[0] * SLOT, (places[-1] + 1) * SLOT)]
        return [(places[i] * SLOT, (places[i + 3] + 1) * SLOT) for i in (0, 4)]

    near = 18 * SLOT
    own_slots = dot(spread[pl.ds(0, near)], normed[tp]).astype(BF16)
    slots[pl.ds(0, near)] = own_slots
    over_sp(slots, arrived, 0, [-d for unit in CHUNKS[0] for d in UNITS[unit]])
    tokens = jnp.concatenate([normed[i] for i in range(TP)], axis=1)
    both = dot_nt(tokens, shared_w[...])
    gate_part, up_part = both[:, :SHARED], both[:, SHARED:]
    units = gate_part * jax.nn.sigmoid(gate_part) * up_part
    shared[tp] = jnp.concatenate([units[: TOK // 2], units[TOK // 2 :]], axis=1).astype(BF16)
    rest = pl.ds(near, PACKED - near)
    slots[rest] = dot(spread[rest], normed[tp]).astype(BF16)
    for chunk in (1, 2):
        over_sp(slots, arrived, chunk, [-d for d in UNITS[chunk + 1]])

    gathers = {"g0": gather(1, shared, (32, 64, 96))}
    gathers["g0"].start()
    mine, mine_end = BACK * SLOT, (BACK + 1) * SLOT
    ins, mids = (in0, in1, in2), (mid0, mid1, mid2)

    def rows_of(buf, own_rows, first_row, end):
        parts = [(first_row, mine), (mine, mine_end), (mine_end, end)]
        if not first_row <= mine < end:
            parts = [(first_row, end)]
        parts = [(lo, hi) for lo, hi in parts if lo < hi]
        return [own_rows if lo == mine else buf[pl.ds(lo, hi - lo)] for lo, hi in parts]

    def begin(chunk):
        over_sp_all(arrived, chunk, 15 if chunk == 0 else 8).wait_recv()
        parts = [
            part
            for unit in CHUNKS[chunk]
            for first_row, end in runs(unit)
            for part in rows_of(arrived, own_slots[mine:mine_end], first_row, end)
        ]
        count = len(CHUNKS[chunk])
        tight = squeeze[pl.ds(0, count * ROWS), pl.ds(0, count * WIDE)]
        ins[chunk][tp] = dot(tight, jnp.concatenate(parts, axis=0)).astype(BF16)
        gathers["i" + str(chunk)] = gather(2 + chunk, ins[chunk], CUTS[chunk], relay=True)
        gathers["i" + str(chunk)].start()

    def run_expert(chunk):
        for i in range(len(CHUNKS[chunk])):
            rows = pl.ds(i * ROWS, ROWS)
            u = jnp.concatenate([ins[chunk][j, rows] for j in range(TP)], axis=1)
            both = dot(u, expert_w[...])
            gate_part = both[:, :LANES]
            value = gate_part * jax.nn.sigmoid(gate_part) * both[:, LANES:]
            mids[chunk][tp, rows] = value.astype(BF16)
        gathers["h" + str(chunk)] = gather(5 + chunk, mids[chunk], CUTS[chunk])
        gathers["h" + str(chunk)].start()

    def run_down(chunk):
        if chunk == 1:
            all_of(down_w, 1).wait_recv()
        for i, unit in enumerate(CHUNKS[chunk]):
            units = [mids[chunk][j, pl.ds(i * ROWS, ROWS)] for j in range(TP)]
            result = dot(jnp.concatenate(units, axis=1), down_w[...].reshape(D, LANES))
            result = dot(widen[...], result.astype(BF16)).astype(BF16)
            done = 0
            for first_row, end in runs(unit):
                back[pl.ds(first_row, end - first_row)] = result[done : done + end - first_row]
                done += end - first_row
            over_sp(back, returned, 3 + unit, UNITS[unit])

    for op in [op for line in ORDER for op in line.split()]:
        if op[0] == "z":
            begin(int(op[1]))
        elif op[0] == "s":

            @pl.loop(1, TP)
            def _(d):
                source = sdown_hbm.at[:, columns(d)]
                remote(source, sdown_w.at[tp], t_send.at[2], t_recv.at[2], tp=tp_at(d)).start()

        else:
            gathers[op[:2]].stage(int(op[2]))
            if op[0] == "i" and op[2] == "5":
                run_expert(int(op[1]))
            elif op[0] == "h" and op[2] == "5":
                run_down(int(op[1]))

    all_of(sdown_w, 2).wait_recv()
    shared_units = jnp.concatenate([shared[i] for i in range(TP)], axis=1)
    nothing = jnp.zeros((SHARED, LANES), BF16)
    parts = [sdown_w[i] for i in range(TP)]
    low = jnp.concatenate([r for part in parts for r in (part, nothing)], axis=0)
    high = jnp.concatenate([r for part in parts for r in (nothing, part)], axis=0)
    shared_out = jnp.concatenate([dot(shared_units, low), dot(shared_units, high)], axis=0)
    base = RESIDUAL_SCALE * normed[tp].astype(F32) + shared_out

    for unit in (2, 3, 0, 1):
        over_sp_all(returned, 3 + unit, 7 if unit == 1 else 8).wait_recv()
    got = jnp.concatenate(rows_of(returned, back[pl.ds(mine, SLOT)], 0, PACKED), axis=0)
    second = base + (dot(picks_hi[...], got) + dot(picks_lo[...], got))

    lane = iota((TOK, LANES), 1)
    total = jnp.sum(second, axis=1, keepdims=True)
    squares = jnp.sum(second * second, axis=1, keepdims=True)
    both = jnp.where(lane == 0, total, jnp.where(lane == 1, squares, 0.0))
    stats[tp] = jnp.transpose(both)[:2]

    @pl.loop(1, TP)
    def _(d):
        to_all(stats, 3)(d).start()

    all_of(stats, 3).wait_recv()
    sums = stats[0]
    for i in range(1, TP):
        sums += stats[i]
    sums = jnp.transpose(jnp.concatenate([sums, jnp.zeros((6, TOK), F32)], axis=0))
    mean = sums[:, 0:1] / D
    var = sums[:, 1:2] / D - mean * mean
    settled = (second - mean) * lax.rsqrt(var + NORM_EPS)
    out[...] = (settled * gain2[...] + bias2[...]).astype(BF16)

    tail.wait_send()
    tail_docs.wait_send()
    for g in (g1, *gathers.values()):
        g.drain()
    for number, ref in enumerate((halo, down_w, sdown_w, stats)):
        all_of(ref, number).wait_send()
    for number, blocks in enumerate((15, 8, 8, 8, 7, 8, 8)):
        over_sp_all(slots if number < 3 else back, number, blocks).wait_send()


def shards(
    layer_input, doc_ids, routes, route_weight, pool_weight, pool_scale, norm1_gain, norm1_bias,
    expert_gate, expert_up, expert_down, shared_gate, shared_up, shared_down, norm2_gain, norm2_bias,
):
    vmem = pl.BlockSpec(memory_space=pltpu.VMEM)
    hbm = pl.BlockSpec(memory_space=pl.ANY)
    dma = pltpu.SemaphoreType.DMA
    scratch = [
        pltpu.VMEM((1, TOK), jnp.int32),
        pltpu.VMEM((2, TOK), jnp.int32),
        pltpu.VMEM((2, TOK), F32),
        *[pltpu.VMEM((1, D), F32)] * 3,
        *[pltpu.VMEM((1, LANES), F32)] * 2,
        pltpu.VMEM((TP, TOK, LANES), BF16),
        pltpu.VMEM((TP, HALO, LANES), BF16),
        pltpu.VMEM((1, LANES), jnp.int32),
        pltpu.VMEM((4, TOK, GROUP), F32),
        pltpu.VMEM((TP, TOK, LANES), BF16),
        pltpu.VMEM((PADDED, LANES), BF16),
        pltpu.VMEM((PADDED, LANES), BF16),
        *[pltpu.VMEM((TP, n * ROWS, LANES), BF16) for n in (2, 1, 1) * 2],
        pltpu.VMEM((TP, TOK // 2, LANES), BF16),
        pltpu.VMEM((PADDED, LANES), BF16),
        pltpu.VMEM((PADDED, LANES), BF16),
        pltpu.VMEM((TP, 2, TOK), F32),
        pltpu.VMEM((4, GROUP, GROUP), BF16),
        pltpu.VMEM((D, 2 * LANES), BF16),
        pltpu.VMEM((2 * SHARED, D), BF16),
        pltpu.VMEM((TP, LANES, LANES), BF16),
        pltpu.VMEM((TP, SHARED, LANES), BF16),
        pltpu.VMEM((4, TOK, TOK), BF16),
        pltpu.VMEM((PACKED, TOK), BF16),
        pltpu.VMEM((TOK, PACKED), BF16),
        pltpu.VMEM((TOK, PACKED), BF16),
        pltpu.VMEM((2 * ROWS, 2 * WIDE), BF16),
        pltpu.VMEM((WIDE, ROWS), BF16),
        dma((16,)),
    ]
    scratch += [dma((8,)), dma((8, 6)), dma((7,)), dma((7,)), dma((6,)), dma((6,))]
    return pl.pallas_call(
        layer,
        out_shape=jax.ShapeDtypeStruct((TOK, LANES), BF16),
        in_specs=[hbm] * 16,
        out_specs=vmem,
        scratch_shapes=scratch,
        compiler_params=pltpu.CompilerParams(
            collective_id=0, has_side_effects=True, vmem_limit_bytes=60 * 1024 * 1024
        ),
    )(
        doc_ids.reshape(1, TOK), routes.T, route_weight.T,
        pool_scale.reshape(1, D), norm1_gain.reshape(1, D), norm1_bias.reshape(1, D),
        norm2_gain.reshape(1, LANES), norm2_bias.reshape(1, LANES),
        layer_input, pool_weight, expert_gate, expert_up, expert_down,
        shared_gate.T, shared_up.T, shared_down,
    )


def solution(mesh):
    placed = (
        P("sp", "tp"), P("sp"), P("sp", None), P("sp", None), P(), P(), P(), P(),
        P("sp", None, "tp"), P("sp", None, "tp"), P("sp", "tp", None),
        P(None, "tp"), P(None, "tp"), P("tp", None), P("tp"), P("tp"),
    )
    return jax.shard_map(
        shards, mesh=mesh, in_specs=placed, out_specs=P("sp", "tp"), check_vma=False
    )
```

```python
import functools

import jax
import jax.numpy as jnp
from jax import lax
from jax.experimental import pallas as pl
from jax.experimental.pallas import tpu as pltpu
from jax.sharding import PartitionSpec as P

MESH = pl.DeviceIdType.MESH
WINDOWS = (2, 4, 8, 16)
RESIDUAL_SCALE = 2.0**0.5
NORM_EPS = 1e-05

SP = 32
TP = 16
TOK = 256
LANES = 128
D = 2048
GROUP = 512
HALO = 16
SHARED = 64
CAP = 22
SLOT = 24
PACKED = SP * SLOT
PADDED = PACKED + 8
BACK = 8
UNITS = (
    tuple(range(-8, 0)),
    tuple(range(0, 8)),
    tuple(range(8, 12)) + tuple(range(-12, -8)),
    tuple(range(12, 20)),
)
CHUNKS = ((0, 1), (2,), (3,))
ROWS = 8 * CAP
WIDE = 8 * SLOT
CUTS = ((96, 176, 272), (48, 96, 144), (48, 80, 128))
ORDER = (
    "g00 g01 g02 s0",
    "z0 g03 z1 i00",
    "g04 i01 i02 i10",
    "i11 i12 z2 i03",
    "i04 i13 i14 i20",
    "i22 i05 i15 i25",
    "g05 h10 h11 h12",
    "h20 h21 h22 h13",
    "h14 h00 h23 h01",
    "h02 h24 h15 h03",
    "h25 h04 h05",
)

F32 = jnp.float32
BF16 = jnp.bfloat16


def iota(shape, dim):
    return lax.broadcasted_iota(jnp.int32, shape, dim)


def dot(a, b):
    return jnp.dot(a, b, preferred_element_type=F32)


def dot_nt(a, b):
    return lax.dot_general(a, b, (((1,), (1,)), ((), ())), preferred_element_type=F32)


class Gather:
    def __init__(self, buf, cuts, tp, send_sem, recv_sem, relay=False):
        self.buf, self.tp, self.relay = buf, tp, relay
        c0, c1, c2 = cuts
        end = buf.shape[1]
        whole = (pl.ds(0, c1), pl.ds(c1, end - c1))
        low = (pl.ds(0, c0), pl.ds(c1, c2 - c1))
        high = (pl.ds(c0, c1 - c0), pl.ds(c2, end - c2))
        self.parts = {"all": whole, "lo": low, "hi": high}
        self.send_sem, self.recv_sem = send_sem, recv_sem

    def at(self, colour, a, b):
        y, x = self.tp // 4, lax.rem(self.tp, 4)
        dx, dy = (a, b) if colour == 0 else (b, a)
        return lax.rem(y + dy + 4, 4) * 4 + lax.rem(x + dx + 4, 4)

    def copy(self, ref, number, to):
        return pltpu.make_async_remote_copy(
            src_ref=ref,
            dst_ref=ref,
            send_sem=self.send_sem.at[0],
            recv_sem=self.recv_sem.at[number],
            device_id={"tp": to},
            device_id_type=MESH,
        )

    def send(self, number, colour, block, to, part="all"):
        self.copy(self.buf.at[block, self.parts[part][colour]], number, to).start()

    def onward(self, number, *sources):
        for b in (1, -1) if self.relay else (1, -1, 2):
            for a in sources:
                for c in (0, 1):
                    where = number if self.relay else 5
                    self.send(where, c, self.at(c, a, 0), self.at(c, 0, b))

    def opposite(self, *sources):
        for way, part in ((1, "lo"), (-1, "hi")):
            for a in sources:
                for c in (0, 1):
                    self.send(5, c, self.at(c, a, -way), self.at(c, 0, way), part)

    def start(self):
        for number, ways in ((0, (1, -1)), (2, (2,))):
            for a in ways:
                for c in (0, 1):
                    self.send(number, c, self.tp, self.at(c, a, 0))
        self.onward(1, 0)

    def stage(self, number):
        blocks = (2, 2, 1, 4, 2, 4 if self.relay else 12)[number]
        self.copy(self.buf.at[pl.ds(0, blocks)], number, self.at(0, 1, 0)).wait_recv()
        if number == 0:
            self.onward(3, -1, 1)
        elif number == 1:
            self.opposite(0)
        elif number == 2:
            self.onward(4, 2)
        elif number == 3:
            self.opposite(-1, 1)
        elif number == 4:
            self.opposite(2)

    def drain(self):
        self.copy(self.buf.at[pl.ds(0, 15)], 0, self.at(0, 1, 0)).wait_send()


def layer(
    docs_hbm, routes_hbm, weights_hbm, scale_hbm, gain1_hbm, bias1_hbm, gain2_hbm, bias2_hbm,
    x_hbm, pool_hbm, gate_hbm, up_hbm, down_hbm, sgate_hbm, sup_hbm, sdown_hbm,
    out,
    docs, routes, weights, scale, gain1, bias1, gain2, bias2,
    x_buf, halo, halo_docs, first, normed, slots, arrived,
    in0, in1, in2, mid0, mid1, mid2, shared, back, returned, stats,
    pool_w, expert_w, shared_w, down_w, sdown_w,
    bands, spread, picks_hi, picks_lo, squeeze, widen,
    load_sem, g_send, g_recv, z_send, z_recv, t_send, t_recv,
):
    sp, tp = lax.axis_index("sp"), lax.axis_index("tp")

    def sp_at(d):
        return lax.rem(sp + d + SP, SP)

    def tp_at(d):
        return lax.rem(tp + d, TP)

    barrier = pltpu.get_barrier_semaphore()

    def greet_sp(d):
        pl.semaphore_signal(barrier, 1, device_id={"sp": sp_at(d)}, device_id_type=MESH)

    pl.loop(9, 24)(greet_sp)

    @pl.loop(1, TP)
    def _(d):
        pl.semaphore_signal(barrier, 1, device_id={"tp": tp_at(d)}, device_id_type=MESH)

    pl.loop(1, 9)(greet_sp)
    pl.loop(24, SP)(greet_sp)

    loads = [
        (docs_hbm, docs), (routes_hbm, routes), (weights_hbm, weights),
        (x_hbm, x_buf.at[tp]),
        (pool_hbm, pool_w),
        (gate_hbm.at[0], expert_w.at[:, pl.ds(0, LANES)]),
        (up_hbm.at[0], expert_w.at[:, pl.ds(LANES, LANES)]),
        (sgate_hbm, shared_w.at[pl.ds(0, SHARED)]),
        (sup_hbm, shared_w.at[pl.ds(SHARED, SHARED)]),
        (down_hbm.at[0, :, pl.ds(pl.multiple_of(tp * LANES, LANES), LANES)], down_w.at[tp]),
        (sdown_hbm.at[:, pl.ds(pl.multiple_of(tp * LANES, LANES), LANES)], sdown_w.at[tp]),
        (scale_hbm, scale), (gain1_hbm, gain1), (bias1_hbm, bias1), (gain2_hbm, gain2), (bias2_hbm, bias2),
    ]
    loads = [pltpu.make_async_copy(s, d, load_sem.at[i]) for i, (s, d) in enumerate(loads)]
    for load in loads:
        load.start()

    for load in loads[:3]:
        load.wait()

    route_rows = routes[...]
    expert = iota((SP, TOK), 0)
    names = [(route_rows[k : k + 1] == expert).astype(F32) for k in (0, 1)]
    before = (iota((TOK, TOK), 0) < iota((TOK, TOK), 1)).astype(F32).astype(BF16)
    rank = dot((names[0] + names[1]).astype(BF16), before)
    order = jnp.bitwise_and(expert - sp + (SP + BACK), SP - 1)
    place = order.astype(F32) * SLOT + rank
    places = [jnp.sum(n * place, axis=0, keepdims=True) for n in names]
    row = iota((PACKED, TOK), 0).astype(F32)
    spread[...] = ((row == places[0]) | (row == places[1])).astype(F32).astype(BF16)
    rows8 = jnp.concatenate(places + [weights[...], jnp.zeros((4, TOK), F32)], axis=0)
    cols = jnp.transpose(rows8)
    column = iota((TOK, PACKED), 1).astype(F32)
    picks = jnp.where(column == cols[:, 0:1], cols[:, 2:3], 0.0)
    picks += jnp.where(column == cols[:, 1:2], cols[:, 3:4], 0.0)
    high = picks.astype(BF16)
    picks_hi[...] = high
    picks_lo[...] = (picks - high.astype(F32)).astype(BF16)

    tight = iota((2 * ROWS, 1), 0).astype(F32)
    tight = tight + 2.0 * jnp.floor((tight + 0.5) * (1.0 / CAP))
    squeeze[...] = (iota((2 * ROWS, 2 * WIDE), 1).astype(F32) == tight).astype(F32).astype(BF16)
    tight = iota((1, ROWS), 1).astype(F32)
    tight = tight + 2.0 * jnp.floor((tight + 0.5) * (1.0 / CAP))
    widen[...] = (iota((WIDE, ROWS), 0).astype(F32) == tight).astype(F32).astype(BF16)

    marks_row = docs[...].astype(F32)
    p, q = iota((TOK, TOK), 0), iota((TOK, TOK), 1)
    marks_col = jnp.sum(jnp.where(p == q, marks_row, 0.0), axis=1, keepdims=True)
    same = (marks_row == marks_col) & (q <= p)
    members = []
    for g, window in enumerate(WINDOWS):
        band = (same & (q > p - window)).astype(F32)
        bands[g] = band.astype(BF16)
        members.append(jnp.sum(band, axis=1, keepdims=True))

    loads[3].wait()
    pl.semaphore_wait(barrier, SP - 1 + TP - 1)

    def remote(src, dst, send_sem, recv_sem, **to):
        return pltpu.make_async_remote_copy(
            src_ref=src, dst_ref=dst, send_sem=send_sem, recv_sem=recv_sem,
            device_id=to, device_id_type=MESH,
        )

    def to_all(ref, number):
        def copy(d):
            return remote(ref.at[tp], ref.at[tp], t_send.at[number], t_recv.at[number], tp=tp_at(d))

        return copy

    def all_of(ref, number):
        block = ref.at[pl.ds(0, TP - 1)]
        return remote(block, block, t_send.at[number], t_recv.at[number], tp=tp_at(1))

    tail = remote(
        x_buf.at[tp, pl.ds(TOK - HALO, HALO)], halo.at[tp], t_send.at[4], t_recv.at[4], sp=sp_at(1)
    )
    tail_docs = remote(docs.at[:, pl.ds(LANES, LANES)], halo_docs, t_send.at[5], t_recv.at[5], sp=sp_at(1))
    tail.start()
    tail_docs.start()
    def gather(number, buf, cuts, relay=False):
        return Gather(buf, cuts, tp, g_send.at[pl.ds(number, 1)], g_recv.at[number], relay)

    g1 = gather(0, x_buf, (64, 128, 192))
    g1.start()
    tail.wait_recv()

    @pl.loop(1, TP)
    def _(d):
        to_all(halo, 0)(d).start()

    tail_docs.wait_recv()
    halo_marks = halo_docs[...][:, LANES - HALO :].astype(F32)
    hp, hq = iota((HALO, HALO), 0), iota((HALO, HALO), 1) - HALO
    halo_same = (halo_marks == marks_col[:HALO]) & (sp > 0)
    g1.stage(0)
    g1.stage(2)

    g1.stage(5)

    def columns(d):
        return pl.ds(pl.multiple_of(tp_at(d) * LANES, LANES), LANES)

    @pl.loop(1, TP)
    def _(d):
        source = down_hbm.at[0, :, columns(d)]
        remote(source, down_w.at[tp], t_send.at[1], t_recv.at[1], tp=tp_at(d)).start()

    for load in loads[4:]:
        load.wait()
    all_of(halo, 0).wait_recv()

    total = jnp.zeros((TOK, 1), F32)
    squares = jnp.zeros((TOK, 1), F32)
    for g, window in enumerate(WINDOWS):
        halo_band = (halo_same & (hq > hp - window)).astype(F32)
        halo_members = members[g][:HALO] + jnp.sum(halo_band, axis=1, keepdims=True)
        share = 1.0 / jnp.concatenate([halo_members, members[g][HALO:]], axis=0)
        values = jnp.concatenate([x_buf[4 * g + i] for i in range(4)], axis=1)
        halo_values = jnp.concatenate([halo[4 * g + i] for i in range(4)], axis=1)
        running = dot(bands[g], values)
        halo_running = running[:HALO] + dot(halo_band.astype(BF16), halo_values)
        running = jnp.concatenate([halo_running, running[HALO:]], axis=0)
        mixed = (running * share - values.astype(F32)).astype(BF16)
        here = pl.ds(g * GROUP, GROUP)
        projected = dot(mixed, pool_w[g]) * scale[:, here]
        value = RESIDUAL_SCALE * values.astype(F32) + projected
        first[g] = value
        total += jnp.sum(value, axis=1, keepdims=True)
        squares += jnp.sum(value * value, axis=1, keepdims=True)
    mean = total / D
    factor = lax.rsqrt(squares / D - mean * mean + NORM_EPS)
    for g in range(4):
        here = pl.ds(g * GROUP, GROUP)
        value = ((first[g] - mean) * factor * gain1[:, here] + bias1[:, here]).astype(BF16)
        for i in range(4):
            normed[4 * g + i] = value[:, i * LANES : (i + 1) * LANES]

    def block(d):
        return pl.ds((d + BACK) % SP * SLOT, SLOT)

    def over_sp(source, target, number, ds):
        for d in ds:
            if d != 0:
                remote(
                    source.at[block(d)], target.at[block(-d)],
                    z_send.at[number], z_recv.at[number], sp=sp_at(d),
                ).start()

    def over_sp_all(ref, number, blocks):
        rows = ref.at[pl.ds(0, blocks * SLOT)]
        return remote(rows, rows, z_send.at[number], z_recv.at[number], sp=sp_at(1))

    def runs(unit):
        places = [(d + BACK) % SP for d in UNITS[unit]]
        if places[-1] - places[0] == 7:
            return [(places[0] * SLOT, (places[-1] + 1) * SLOT)]
        return [(places[i] * SLOT, (places[i + 3] + 1) * SLOT) for i in (0, 4)]

    near = 18 * SLOT
    own_slots = dot(spread[pl.ds(0, near)], normed[tp]).astype(BF16)
    slots[pl.ds(0, near)] = own_slots
    over_sp(slots, arrived, 0, [-d for unit in CHUNKS[0] for d in UNITS[unit]])
    tokens = jnp.concatenate([normed[i] for i in range(TP)], axis=1)
    both = dot_nt(tokens, shared_w[...])
    gate_part, up_part = both[:, :SHARED], both[:, SHARED:]
    units = gate_part * jax.nn.sigmoid(gate_part) * up_part
    shared[tp] = jnp.concatenate([units[: TOK // 2], units[TOK // 2 :]], axis=1).astype(BF16)
    rest = pl.ds(near, PACKED - near)
    slots[rest] = dot(spread[rest], normed[tp]).astype(BF16)
    for chunk in (1, 2):
        over_sp(slots, arrived, chunk, [-d for d in UNITS[chunk + 1]])

    gathers = {"g0": gather(1, shared, (32, 64, 96), relay=True)}
    gathers["g0"].start()
    mine, mine_end = BACK * SLOT, (BACK + 1) * SLOT
    ins, mids = (in0, in1, in2), (mid0, mid1, mid2)

    def rows_of(buf, own_rows, first_row, end):
        parts = [(first_row, mine), (mine, mine_end), (mine_end, end)]
        if not first_row <= mine < end:
            parts = [(first_row, end)]
        parts = [(lo, hi) for lo, hi in parts if lo < hi]
        return [own_rows if lo == mine else buf[pl.ds(lo, hi - lo)] for lo, hi in parts]

    def begin(chunk):
        over_sp_all(arrived, chunk, 15 if chunk == 0 else 8).wait_recv()
        parts = [
            part
            for unit in CHUNKS[chunk]
            for first_row, end in runs(unit)
            for part in rows_of(arrived, own_slots[mine:mine_end], first_row, end)
        ]
        count = len(CHUNKS[chunk])
        tight = squeeze[pl.ds(0, count * ROWS), pl.ds(0, count * WIDE)]
        ins[chunk][tp] = dot(tight, jnp.concatenate(parts, axis=0)).astype(BF16)
        gathers["i" + str(chunk)] = gather(2 + chunk, ins[chunk], CUTS[chunk], relay=chunk < 2)
        gathers["i" + str(chunk)].start()

    def run_expert(chunk):
        for i in range(len(CHUNKS[chunk])):
            rows = pl.ds(i * ROWS, ROWS)
            u = jnp.concatenate([ins[chunk][j, rows] for j in range(TP)], axis=1)
            both = dot(u, expert_w[...])
            gate_part = both[:, :LANES]
            value = gate_part * jax.nn.sigmoid(gate_part) * both[:, LANES:]
            mids[chunk][tp, rows] = value.astype(BF16)
        gathers["h" + str(chunk)] = gather(5 + chunk, mids[chunk], CUTS[chunk], relay=True)
        gathers["h" + str(chunk)].start()

    def run_down(chunk):
        if chunk == 1:
            all_of(down_w, 1).wait_recv()
        for i, unit in enumerate(CHUNKS[chunk]):
            units = [mids[chunk][j, pl.ds(i * ROWS, ROWS)] for j in range(TP)]
            result = dot(jnp.concatenate(units, axis=1), down_w[...].reshape(D, LANES))
            result = dot(widen[...], result.astype(BF16)).astype(BF16)
            done = 0
            for first_row, end in runs(unit):
                back[pl.ds(first_row, end - first_row)] = result[done : done + end - first_row]
                done += end - first_row
            over_sp(back, returned, 3 + unit, UNITS[unit])

    for op in [op for line in ORDER for op in line.split()]:
        if op[0] == "z":
            begin(int(op[1]))
        elif op[0] == "s":

            @pl.loop(1, TP)
            def _(d):
                source = sdown_hbm.at[:, columns(d)]
                remote(source, sdown_w.at[tp], t_send.at[2], t_recv.at[2], tp=tp_at(d)).start()

        else:
            gathers[op[:2]].stage(int(op[2]))
            if op[0] == "i" and op[2] == "5":
                run_expert(int(op[1]))
            elif op[0] == "h" and op[2] == "5":
                run_down(int(op[1]))

    all_of(sdown_w, 2).wait_recv()
    shared_units = jnp.concatenate([shared[i] for i in range(TP)], axis=1)
    nothing = jnp.zeros((SHARED, LANES), BF16)
    parts = [sdown_w[i] for i in range(TP)]
    low = jnp.concatenate([r for part in parts for r in (part, nothing)], axis=0)
    high = jnp.concatenate([r for part in parts for r in (nothing, part)], axis=0)
    shared_out = jnp.concatenate([dot(shared_units, low), dot(shared_units, high)], axis=0)
    base = RESIDUAL_SCALE * normed[tp].astype(F32) + shared_out

    for unit in (2, 3, 0, 1):
        over_sp_all(returned, 3 + unit, 7 if unit == 1 else 8).wait_recv()
    got = jnp.concatenate(rows_of(returned, back[pl.ds(mine, SLOT)], 0, PACKED), axis=0)
    second = base + (dot(picks_hi[...], got) + dot(picks_lo[...], got))

    lane = iota((TOK, LANES), 1)
    total = jnp.sum(second, axis=1, keepdims=True)
    squares = jnp.sum(second * second, axis=1, keepdims=True)
    both = jnp.where(lane == 0, total, jnp.where(lane == 1, squares, 0.0))
    stats[tp] = jnp.transpose(both)[:2]

    @pl.loop(1, TP)
    def _(d):
        to_all(stats, 3)(d).start()

    all_of(stats, 3).wait_recv()
    sums = stats[0]
    for i in range(1, TP):
        sums += stats[i]
    sums = jnp.transpose(jnp.concatenate([sums, jnp.zeros((6, TOK), F32)], axis=0))
    mean = sums[:, 0:1] / D
    var = sums[:, 1:2] / D - mean * mean
    settled = (second - mean) * lax.rsqrt(var + NORM_EPS)
    out[...] = (settled * gain2[...] + bias2[...]).astype(BF16)

    tail.wait_send()
    tail_docs.wait_send()
    for g in (g1, *gathers.values()):
        g.drain()
    for number, ref in enumerate((halo, down_w, sdown_w, stats)):
        all_of(ref, number).wait_send()
    for number, blocks in enumerate((15, 8, 8, 8, 7, 8, 8)):
        over_sp_all(slots if number < 3 else back, number, blocks).wait_send()


def shards(
    layer_input, doc_ids, routes, route_weight, pool_weight, pool_scale, norm1_gain, norm1_bias,
    expert_gate, expert_up, expert_down, shared_gate, shared_up, shared_down, norm2_gain, norm2_bias,
):
    vmem = pl.BlockSpec(memory_space=pltpu.VMEM)
    hbm = pl.BlockSpec(memory_space=pl.ANY)
    dma = pltpu.SemaphoreType.DMA
    scratch = [
        pltpu.VMEM((1, TOK), jnp.int32),
        pltpu.VMEM((2, TOK), jnp.int32),
        pltpu.VMEM((2, TOK), F32),
        *[pltpu.VMEM((1, D), F32)] * 3,
        *[pltpu.VMEM((1, LANES), F32)] * 2,
        pltpu.VMEM((TP, TOK, LANES), BF16),
        pltpu.VMEM((TP, HALO, LANES), BF16),
        pltpu.VMEM((1, LANES), jnp.int32),
        pltpu.VMEM((4, TOK, GROUP), F32),
        pltpu.VMEM((TP, TOK, LANES), BF16),
        pltpu.VMEM((PADDED, LANES), BF16),
        pltpu.VMEM((PADDED, LANES), BF16),
        *[pltpu.VMEM((TP, n * ROWS, LANES), BF16) for n in (2, 1, 1) * 2],
        pltpu.VMEM((TP, TOK // 2, LANES), BF16),
        pltpu.VMEM((PADDED, LANES), BF16),
        pltpu.VMEM((PADDED, LANES), BF16),
        pltpu.VMEM((TP, 2, TOK), F32),
        pltpu.VMEM((4, GROUP, GROUP), BF16),
        pltpu.VMEM((D, 2 * LANES), BF16),
        pltpu.VMEM((2 * SHARED, D), BF16),
        pltpu.VMEM((TP, LANES, LANES), BF16),
        pltpu.VMEM((TP, SHARED, LANES), BF16),
        pltpu.VMEM((4, TOK, TOK), BF16),
        pltpu.VMEM((PACKED, TOK), BF16),
        pltpu.VMEM((TOK, PACKED), BF16),
        pltpu.VMEM((TOK, PACKED), BF16),
        pltpu.VMEM((2 * ROWS, 2 * WIDE), BF16),
        pltpu.VMEM((WIDE, ROWS), BF16),
        dma((16,)),
    ]
    scratch += [dma((8,)), dma((8, 6)), dma((7,)), dma((7,)), dma((6,)), dma((6,))]
    return pl.pallas_call(
        layer,
        out_shape=jax.ShapeDtypeStruct((TOK, LANES), BF16),
        in_specs=[hbm] * 16,
        out_specs=vmem,
        scratch_shapes=scratch,
        compiler_params=pltpu.CompilerParams(
            collective_id=0, has_side_effects=True, vmem_limit_bytes=60 * 1024 * 1024
        ),
    )(
        doc_ids.reshape(1, TOK), routes.T, route_weight.T,
        pool_scale.reshape(1, D), norm1_gain.reshape(1, D), norm1_bias.reshape(1, D),
        norm2_gain.reshape(1, LANES), norm2_bias.reshape(1, LANES),
        layer_input, pool_weight, expert_gate, expert_up, expert_down,
        shared_gate.T, shared_up.T, shared_down,
    )


def solution(mesh):
    placed = (
        P("sp", "tp"), P("sp"), P("sp", None), P("sp", None), P(), P(), P(), P(),
        P("sp", None, "tp"), P("sp", None, "tp"), P("sp", "tp", None),
        P(None, "tp"), P(None, "tp"), P("tp", None), P("tp"), P("tp"),
    )
    return jax.shard_map(
        shards, mesh=mesh, in_specs=placed, out_specs=P("sp", "tp"), check_vma=False
    )
```
